256 devices in a mesh: ep: 64 (over z, x, core), tp: 4 (over y).
Axes of the slice: x: 4, y: 4, z: 8, core: 2. Of those that a mesh axis runs over, the one named last changes fastest.
Arguments:
- conv_input: bfloat16 [65536, 2048], P('ep', 'tp'), may hold values from -6 to 6
- conv_kernel: bfloat16 [31, 2048], P(None, 'tp'), may hold values from -2 to 2
- norm_gain: float32 [2048], P('tp'), may hold values from 0.1 to 1.9
- norm_shift: float32 [2048], P('tp'), may hold values from -3 to 3
- conv_proj: bfloat16 [2048, 2048], P('tp'), may hold values from -0.125 to 0.125
- moe_input: bfloat16 [16384, 2048], P(('ep', 'tp')), may hold values from -6 to 6
- moe_gain: float32 [2048], replicated, may hold values from 0.1 to 1.9
- routes: int32 [16384, 2], P('ep'), may hold values from 0 to 63, all different within a row; in each aligned block of 256 rows (0 to 255, 256 to 511, ...) at most 16 rows name the same one
- route_weights: float32 [16384, 2], P('ep'), may hold values from 0.2 to 1
- gate_proj: bfloat16 [64, 2048, 2048], P('ep', None, 'tp'), may hold values from -0.125 to 0.125
- up_proj: bfloat16 [64, 2048, 2048], P('ep', None, 'tp'), may hold values from -0.125 to 0.125
- down_proj: bfloat16 [64, 2048, 2048], P('ep', 'tp'), may hold values from -0.125 to 0.125
Outputs:
- conv_out: bfloat16 [65536, 2048], P(('ep', 'tp'))
- moe_out: bfloat16 [16384, 2048], P(('ep', 'tp'))
The draws below stay inside these ranges and needn't reach their ends.
Inputs may be any that keep to these rules, and one draw needn't show every extreme that they name: `routes`: each row names 2 different experts. In each aligned block of 256 rows no expert is named by more than 16 rows, and in some blocks an expert is named by exactly 16 rows.
All inputs are finite; a program needn't handle non-finite values.
Results may differ from the reference program's by a relative error of at most 0.012.
Values may be sent and summed in bfloat16 or wider, within the bound.
A program may use at most 128 MiB of HBM per device.

```python
import math
import jax
import jax.numpy as jnp
import numpy as np
from jax import lax

D = 2048
FE = 2048
CONV_WIDTH = 31
TOPK = 2
TOK_DEV = 64
EXPERTS = 64
CAPG = 16
CONV_TOKENS = 65536
MOE_TOKENS = 16384
N_EP = 64
N_TP = 4


def draw_conv_kernel(key, part):
    first_key, second_key = jax.random.split(jax.random.fold_in(key, 11))
    factors = jax.random.permutation(first_key, jnp.array([0.5, 0.9, 1.6, 2.6], jnp.float32))
    channel_block = jnp.arange(D, dtype=jnp.int32) * 4 // D
    column_scale = factors[channel_block] / math.sqrt(CONV_WIDTH)
    base = jnp.clip(jax.random.normal(second_key, (CONV_WIDTH, D), jnp.float32), -4.0, 4.0)
    return (base * column_scale[None, :]).astype(jnp.bfloat16)


def shard_levels(stream_key, extent, cuts, least, top_value):
    def one(axis_at, parts):
        heights = jax.random.uniform(jax.random.fold_in(jax.random.fold_in(stream_key, 6), axis_at), (parts,), jnp.float32, least / len(cuts), top_value / len(cuts))
        return jnp.repeat(jnp.exp(heights), extent[axis_at] // parts).reshape((-1,) + (1,) * (len(extent) - axis_at - 1))

    factor_of = one(*cuts[0])
    for cut in cuts[1:]:
        factor_of = factor_of * one(*cut)
    return factor_of


def assign_block(own_key, own, number, rows, number_of, top, most, slope):
    ranking = jax.random.permutation(own_key, number_of)
    packed, usual = load_shares(number_of, rows * top, most, slope, True), load_shares(number_of, rows * top, most, slope, False)
    places = jnp.arange(number_of)

    def named(sizes, offset_by):
        used = int((sizes > 0).sum())
        fixed = max(1, used // 4)
        moved = fixed + (places - fixed + offset_by * (used - fixed)) % max(1, number_of - fixed)
        return jnp.zeros((number_of,), jnp.int32).at[ranking[jnp.where(places < fixed, places, moved)]].set(jnp.asarray(sizes, jnp.int32))

    sizes = jnp.where(number % 4 == 0, named(packed, number // 4), named(usual, number - number // 4 - 1))
    mixed = jax.random.permutation(jax.random.fold_in(own, 3), number_of)
    giver, taker = mixed[0:number_of // 2 * 2:2], mixed[1:number_of // 2 * 2:2]
    slack = jnp.minimum(sizes[giver] - 1, most - sizes[taker]) // 2
    slack = jnp.where((giver == ranking[0]) | (taker == ranking[0]) | (sizes[taker] == 0), 0, jnp.maximum(slack, 0))
    moved = jax.random.randint(jax.random.fold_in(own, 4), (number_of // 2,), 0, 1 << 20) % (slack + 1)
    sizes = sizes.at[giver].add(-moved).at[taker].add(moved)
    labels = jnp.searchsorted(jnp.cumsum(sizes), jnp.arange(rows * top), side="right").astype(jnp.int32)
    listing = labels.reshape(top, rows).T
    listing = listing[jax.random.permutation(jax.random.fold_in(own, 1), rows)]
    offset_by = jax.random.randint(jax.random.fold_in(own, 2), (rows, 1), 0, top)
    return jnp.take_along_axis(listing, (jnp.arange(top)[None, :] + offset_by) % top, axis=1)


def load_shares(amount, total, most, slope, full):
    portions = [(1 << 20) // math.isqrt(standing ** slope) + 1 for standing in range(1, amount + 1)]
    largest = most if full else min(most, max(-(-total // amount), total * portions[0] // sum(portions)))
    least = 1 if total - largest >= amount - 1 else 0
    counts, rest = [largest] + [least] * (amount - 1), total - largest - least * (amount - 1)
    while rest > 0:
        candidates = [i for i in range(1, amount) if counts[i] < largest] or [i for i in range(1, amount) if counts[i] < most]
        whole, left = sum([portions[i] for i in candidates]), rest
        for i in candidates:
            more = min(most - counts[i], max(1, left * portions[i] // whole), rest)
            counts[i] = counts[i] + more
            rest = rest - more
    return np.array(counts)


def noise(stream_key, extent, scale, limit, cuts=(), held_as=jnp.bfloat16):
    gain = shard_levels(stream_key, extent, cuts, -0.22, 0.18) if cuts else 1.0
    entries = jax.random.normal(stream_key, extent, jnp.float32) * scale * gain
    return jnp.minimum(jnp.maximum(entries, -limit), limit).astype(held_as)


def setup_inputs(seed: int = 0) -> dict:
    splits = jax.random.split(jax.random.key(seed), 13)
    conv_input = noise(splits[0], (CONV_TOKENS, D), 1.0, 6.0, ((0, 64), (1, 4)))
    conv_kernel = draw_conv_kernel(jax.random.fold_in(splits[12], 71), 0)
    norm_gain = jnp.clip(1.0 + 0.18 * jax.random.normal(splits[2], (D,), jnp.float32), 0.1, 1.9)
    norm_shift = noise(splits[3], (D,), 0.5, 3.0, ((0, 4),), jnp.float32)
    conv_proj = noise(splits[4], (D, D), D ** -0.5, 0.125, ((0, 4),))
    moe_input = noise(splits[5], (MOE_TOKENS, D), 1.0, 6.0, ((0, 256),))
    moe_gain = jnp.clip(1.0 + 0.18 * jax.random.normal(splits[6], (D,), jnp.float32), 0.1, 1.9)
    routes_keys = jax.random.split(jax.random.fold_in(splits[7], 1), MOE_TOKENS // (N_TP * TOK_DEV))
    routes_turns = jax.random.permutation(jax.random.fold_in(splits[7], 3), MOE_TOKENS // (N_TP * TOK_DEV))
    routes = jax.vmap(lambda own, number: assign_block(jax.random.fold_in(splits[7], 2), own, number, N_TP * TOK_DEV, EXPERTS, TOPK, CAPG, 2))(routes_keys, routes_turns).reshape((MOE_TOKENS, TOPK))
    route_weights = jnp.clip(0.2 + 0.8 * jax.random.uniform(splits[8], (MOE_TOKENS, TOPK), jnp.float32) ** shard_levels(splits[8], (MOE_TOKENS, TOPK), ((0, 64),), -0.2, 0.2), 0.2, 1.0)
    gate_proj = noise(splits[9], (EXPERTS, D, FE), D ** -0.5, 0.125, ((0, 64), (2, 4)))
    up_proj = noise(splits[10], (EXPERTS, D, FE), D ** -0.5, 0.125, ((0, 64), (2, 4)))
    down_proj = noise(splits[11], (EXPERTS, FE, D), FE ** -0.5, 0.125, ((0, 64), (1, 4)))
    return dict(conv_input=conv_input, conv_kernel=conv_kernel, norm_gain=norm_gain, norm_shift=norm_shift, conv_proj=conv_proj, moe_input=moe_input, moe_gain=moe_gain, routes=routes, route_weights=route_weights, gate_proj=gate_proj, up_proj=up_proj, down_proj=down_proj)


def conv_half(conv_input, conv_kernel, norm_gain, norm_shift, conv_proj):
    reach = CONV_WIDTH - 1
    padded = jnp.concatenate([jnp.zeros((reach, D), conv_input.dtype), conv_input], axis=0)
    taps = conv_kernel.astype(jnp.float32)
    mixed = jnp.zeros((CONV_TOKENS, D), jnp.float32)
    for offset in range(CONV_WIDTH):
        mixed = mixed + padded[offset:offset + CONV_TOKENS].astype(jnp.float32) * taps[offset]
    center = lax.optimization_barrier(jnp.sum(mixed, axis=1)) / D
    spread = jnp.maximum(lax.optimization_barrier(jnp.sum(mixed * mixed, axis=1)) / D - center * center, 0.0)
    scaled = (mixed - center[:, None]) * lax.rsqrt(spread[:, None] + 1e-05) * norm_gain + norm_shift
    activated = jax.nn.silu(scaled).astype(jnp.bfloat16)
    block = D // N_TP
    total = jnp.zeros((CONV_TOKENS, D), jnp.float32)
    for part in range(N_TP):
        piece = jnp.dot(activated[:, part * block:(part + 1) * block], conv_proj[part * block:(part + 1) * block], preferred_element_type=jnp.float32)
        total = total + lax.optimization_barrier(piece.astype(jnp.bfloat16)).astype(jnp.float32)
    return total.astype(jnp.bfloat16)

def moe_half(moe_input, moe_gain, routes, route_weights, gate_proj, up_proj, down_proj):
    moe_float = moe_input.astype(jnp.float32)
    normed = (moe_float * lax.rsqrt(lax.optimization_barrier(jnp.mean(moe_float * moe_float, axis=1, keepdims=True)) + 1e-06) * moe_gain).astype(jnp.bfloat16)
    block = FE // N_TP
    slots = N_EP * CAPG

    def one_expert(total, items):
        expert, gate_w, up_w, down_w = items
        hits = routes == expert
        weight = lax.optimization_barrier(jnp.sum(jnp.where(hits, route_weights, 0.0), axis=1))
        named = jnp.any(hits, axis=1)
        index = jnp.nonzero(named, size=slots, fill_value=0)[0].astype(jnp.int32)
        valid = jnp.arange(slots, dtype=jnp.int32) < jnp.sum(named.astype(jnp.int32))
        rows = normed[index]
        result = jnp.zeros((slots, D), jnp.float32)
        for part in range(N_TP):
            low = part * block
            gated = jax.nn.silu(jnp.dot(rows, gate_w[:, low:low + block], preferred_element_type=jnp.float32))
            hidden = (gated * jnp.dot(rows, up_w[:, low:low + block], preferred_element_type=jnp.float32)).astype(jnp.bfloat16)
            piece = jnp.dot(hidden, down_w[low:low + block], preferred_element_type=jnp.float32)
            result = result + lax.optimization_barrier(piece.astype(jnp.bfloat16)).astype(jnp.float32)
        scale = jnp.where(valid, weight[index], 0.0)
        return (total.at[index].add(result * scale[:, None]), None)
    experts = jnp.arange(EXPERTS, dtype=jnp.int32)
    total, _ = lax.scan(one_expert, jnp.zeros((MOE_TOKENS, D), jnp.float32), (experts, gate_proj, up_proj, down_proj))
    return total.astype(jnp.bfloat16)

def reference(conv_input, conv_kernel, norm_gain, norm_shift, conv_proj, moe_input, moe_gain, routes, route_weights, gate_proj, up_proj, down_proj):
    conv_out = conv_half(conv_input, conv_kernel, norm_gain, norm_shift, conv_proj)
    moe_out = moe_half(moe_input, moe_gain, routes, route_weights, gate_proj, up_proj, down_proj)
    return (conv_out, moe_out)
```

```python
import jax
import jax.numpy as jnp
from jax import lax
from jax.experimental import pallas as pl
from jax.experimental.pallas import tpu as pltpu
from jax.sharding import PartitionSpec as P

MESH = pl.DeviceIdType.MESH
F32 = jnp.float32
BF16 = jnp.bfloat16

EP = 64
TP = 4
D = 2048
BLK = D // TP
GROUP = 256
TOK = GROUP // TP
CAP = 16
SLOTS = EP * CAP
NCH = 4
CROWS = SLOTS // NCH
CSRC = EP // NCH
HALF = CROWS // 2
ROWS = 1024
QROWS = ROWS // TP
HALO = 32
TAPS = 31
RB = 64
NRB = ROWS // RB
NCB = BLK // 128
OWN = 48


def kernel(
    x_hbm, ck_ref, gain_ref, shift_ref, proj_hbm, mi_hbm, mgain_ref, rt_ref, rw_ref, wg_hbm, wu_hbm, wd_hbm,
    co_hbm, mo_hbm,
    xb, xf, ckf, mixed, tst, act, proj, mi, wg, wu, wd, nrm, grp, dsp, xg, hid, part, ha, hb, fa, fb,
    rout, rin, whi, wlo, cmb, mo, cov,
    load_sem, put_sem, halo_sem, grp_send, grp_recv, st_send, st_recv, dsp_send, dsp_recv,
    ag_send, agl, agr, agfl, agfr, rs_send_sem, hal, hbl, fal, fbl, ret_send, ret_recv, fin_send, fin_recv,
):
    g = lax.axis_index("ep")
    y = lax.axis_index("tp")
    right, left, opp = (y + 1) % TP, (y + 3) % TP, (y + 2) % TP
    z, xx, core = g // 8, (g % 8) // 2, g % 2
    ycol = pl.multiple_of(y * BLK, BLK)

    def offsets(i):
        c, j = i // CSRC, i % CSRC
        p = j % 2
        dz = ((c + 1) % 4) * (1 - p) + (7 - c) * p
        return dz, j // 4, (j // 2) % 2

    def ahead(i):
        dz, dx, dc = offsets(i)
        return ((z + dz) % 8) * 8 + ((xx + dx) % 4) * 2 + (core + dc) % 2

    def behind(i):
        dz, dx, dc = offsets(i)
        return ((z + 8 - dz) % 8) * 8 + ((xx + 4 - dx) % 4) * 2 + (core + dc) % 2

    def remote(src, dst, send, recv, ep, tp):
        return pltpu.make_async_remote_copy(
            src_ref=src, dst_ref=dst, send_sem=send, recv_sem=recv, device_id=(ep, tp), device_id_type=MESH
        )

    def landed(ref, sem):
        pltpu.make_async_copy(ref, ref, sem).wait()

    loads = [
        pltpu.make_async_copy(mi_hbm, mi, load_sem.at[0]),
        pltpu.make_async_copy(x_hbm, xb.at[pl.ds(HALO, ROWS)], load_sem.at[1]),
        pltpu.make_async_copy(proj_hbm, proj, load_sem.at[2]),
        pltpu.make_async_copy(wg_hbm.at[0], wg, load_sem.at[3]),
        pltpu.make_async_copy(wu_hbm.at[0], wu, load_sem.at[4]),
        pltpu.make_async_copy(wd_hbm.at[0], wd, load_sem.at[5]),
    ]
    for load in loads:
        load.start()

    barrier = pltpu.get_barrier_semaphore()
    for d in range(1, TP):
        pl.semaphore_signal(barrier, inc=1, device_id=(g, (y + d) % TP), device_id_type=MESH)

    def greet(s, carry):
        pl.semaphore_signal(barrier, inc=1, device_id=(ahead(s + s // OWN), y), device_id_type=MESH)
        return carry

    lax.fori_loop(0, EP - 1, greet, 0)

    loads[0].wait()
    rows = mi[...].astype(F32)
    scale = lax.rsqrt(jnp.mean(rows * rows, axis=1, keepdims=True) + 1e-6)
    nrm[...] = (rows * scale * mgain_ref[...]).astype(BF16)
    grp[pl.ds(pl.multiple_of(y * TOK, TOK), TOK), :] = nrm[:, pl.ds(ycol, BLK)]

    loads[1].wait()
    for cb in range(NCB):
        ckf[cb, 0:TAPS, :] = ck_ref[:, cb * 128 : cb * 128 + 128].astype(F32)

    def widen(b, carry):
        r = pl.multiple_of(HALO + b * 64, 32)
        for cb in range(NCB):
            xf[cb, pl.ds(r, 64), :] = xb[pl.ds(r, 64), cb * 128 : cb * 128 + 128].astype(F32)
        return carry

    lax.fori_loop(0, ROWS // 64, widen, 0)

    pl.semaphore_wait(barrier, EP - 1 + TP - 1)

    sends = []
    for d in range(1, TP):
        to = (y + d) % TP
        sends.append(
            remote(
                nrm.at[:, pl.ds(pl.multiple_of(to * BLK, BLK), BLK)],
                grp.at[pl.ds(pl.multiple_of(y * TOK, TOK), TOK), :],
                grp_send.at[d],
                grp_recv.at[d],
                g,
                to,
            )
        )
        sends[-1].start()

    halo = remote(xb.at[pl.ds(ROWS, HALO)], xb.at[pl.ds(0, HALO)], halo_sem.at[0], halo_sem.at[1], (g + 1) % EP, y)

    @pl.when(g < EP - 1)
    def _():
        halo.start()

    lane = lax.broadcasted_iota(jnp.int32, (RB, 128), 1)

    def conv_rows(rb, stats):
        base = pl.multiple_of(rb * RB, RB)
        total = jnp.zeros((RB, 128), F32)
        squares = jnp.zeros((RB, 128), F32)
        for cb in range(NCB):
            acc = jnp.zeros((RB, 128), F32)
            for tap in range(TAPS):
                acc = acc + xf[cb, pl.ds(base + (2 + tap), RB), :] * ckf[cb, tap : tap + 1, :]
            mixed[cb, pl.ds(base, RB), :] = acc
            total = total + acc
            squares = squares + acc * acc
        stats = jnp.where(lane == rb, jnp.sum(total, axis=1, keepdims=True), stats)
        return jnp.where(lane == rb + NRB, jnp.sum(squares, axis=1, keepdims=True), stats)

    stats = lax.fori_loop(1, NRB, conv_rows, jnp.zeros((RB, 128), F32))

    @pl.when(g > 0)
    def _():
        halo.wait_recv()

    @pl.when(g == 0)
    def _():
        xb[0:HALO, :] = jnp.zeros((HALO, BLK), BF16)

    for cb in range(NCB):
        xf[cb, 0:HALO, :] = xb[0:HALO, cb * 128 : cb * 128 + 128].astype(F32)
    stats = conv_rows(0, stats)
    tst[TP] = stats
    stat_sends = []
    for d in range(1, TP):
        to = (y + d) % TP
        stat_sends.append(remote(tst.at[TP], tst.at[y], st_send.at[d], st_recv.at[d], g, to))
        stat_sends[-1].start()

    expert_col = lax.broadcasted_iota(jnp.int32, (EP, GROUP), 0)
    named = (rt_ref[0:1, :] == expert_col) | (rt_ref[1:2, :] == expert_col)
    named_f = jnp.where(named, 1.0, 0.0)
    earlier = lax.broadcasted_iota(jnp.int32, (GROUP, GROUP), 0) < lax.broadcasted_iota(jnp.int32, (GROUP, GROUP), 1)
    rank = jnp.dot(named_f.astype(BF16), jnp.where(earlier, 1.0, 0.0).astype(BF16), preferred_element_type=F32)
    rank = jnp.where(named, rank, -1.0).astype(BF16)
    slot = lax.broadcasted_iota(jnp.int32, (SLOTS, EP), 0)
    spread_rows = jnp.where(slot // CAP == lax.broadcasted_iota(jnp.int32, (SLOTS, EP), 1), 1.0, 0.0).astype(BF16)
    ranks = jnp.dot(spread_rows, rank, preferred_element_type=F32)
    place = (lax.broadcasted_iota(jnp.int32, (SLOTS, GROUP), 0) % CAP).astype(F32)
    chosen = jnp.where(ranks == place, 1.0, 0.0).astype(BF16)
    for d in range(1, TP):
        landed(grp.at[pl.ds(0, TOK), :], grp_recv.at[d])
    dsp[...] = jnp.dot(chosen, grp[...], preferred_element_type=F32).astype(BF16)

    def dispatch(s, carry):
        i = s + s // OWN
        e = ahead(i)
        remote(
            dsp.at[pl.ds(pl.multiple_of(e * CAP, CAP), CAP), :],
            xg.at[pl.ds(pl.multiple_of(i * CAP, CAP), CAP), pl.ds(ycol, BLK)],
            dsp_send,
            dsp_recv.at[i // CSRC],
            e,
            y,
        ).start()
        return carry

    lax.fori_loop(0, EP - 1, dispatch, 0)
    xg[OWN * CAP : OWN * CAP + CAP, pl.ds(ycol, BLK)] = dsp[pl.ds(pl.multiple_of(g * CAP, CAP), CAP), :]

    pick = lax.broadcasted_iota(jnp.int32, (128, GROUP), 0)
    table = jnp.where(pick == 0, rt_ref[0:1, :].astype(F32), 0.0)
    table = jnp.where(pick == 1, rt_ref[1:2, :].astype(F32), table)
    table = jnp.where(pick == 2, rw_ref[0:1, :], table)
    table = jnp.where(pick == 3, rw_ref[1:2, :], table)
    table = jnp.transpose(table)
    expert_lane = lax.broadcasted_iota(jnp.int32, (GROUP, EP), 1).astype(F32)
    first = table[:, 0:1] == expert_lane
    second = table[:, 1:2] == expert_lane
    named_t = jnp.where(first | second, 1.0, 0.0)
    before = lax.broadcasted_iota(jnp.int32, (GROUP, GROUP), 1) < lax.broadcasted_iota(jnp.int32, (GROUP, GROUP), 0)
    rank_t = jnp.dot(jnp.where(before, 1.0, 0.0).astype(BF16), named_t.astype(BF16), preferred_element_type=F32)
    rank_t = jnp.where(first | second, rank_t, -1.0).astype(BF16)
    weight_t = jnp.where(first, table[:, 2:3], 0.0) + jnp.where(second, table[:, 3:4], 0.0)
    weight_hi = weight_t.astype(BF16)
    weight_lo = (weight_t - weight_hi.astype(F32)).astype(BF16)
    slot_lane = lax.broadcasted_iota(jnp.int32, (EP, SLOTS), 1)
    spread_cols = jnp.where(slot_lane // CAP == lax.broadcasted_iota(jnp.int32, (EP, SLOTS), 0), 1.0, 0.0).astype(BF16)
    hit = jnp.dot(rank_t, spread_cols, preferred_element_type=F32) == (
        lax.broadcasted_iota(jnp.int32, (GROUP, SLOTS), 1) % CAP
    ).astype(F32)
    whi[...] = jnp.where(hit, jnp.dot(weight_hi, spread_cols, preferred_element_type=F32), 0.0).astype(BF16)
    wlo[...] = jnp.where(hit, jnp.dot(weight_lo, spread_cols, preferred_element_type=F32), 0.0).astype(BF16)

    for d in range(1, TP):
        landed(tst.at[0], st_recv.at[d])
    means = (tst[TP] + tst[right] + tst[opp] + tst[left]) * (1.0 / D)

    def activate(rb, carry):
        base = pl.multiple_of(rb * RB, RB)
        center = jnp.sum(jnp.where(lane == rb, means, 0.0), axis=1, keepdims=True)
        square = jnp.sum(jnp.where(lane == rb + NRB, means, 0.0), axis=1, keepdims=True)
        inv = lax.rsqrt(jnp.maximum(square - center * center, 0.0) + 1e-5)
        for cb in range(NCB):
            cols = slice(cb * 128, cb * 128 + 128)
            v = (mixed[cb, pl.ds(base, RB), :] - center) * inv * gain_ref[:, cols] + shift_ref[:, cols]
            act[pl.ds(base, RB), cols] = (v / (1.0 + jnp.exp(-v))).astype(BF16)
        return carry

    lax.fori_loop(0, NRB, activate, 0)
    loads[2].wait()

    def rs_pieces(j):
        return (
            (part.at[j, opp, pl.ds(0, HALF)], ha.at[j], hal.at[j], right),
            (part.at[j, opp, pl.ds(HALF, HALF)], hb.at[j], hbl.at[j], left),
            (part.at[j, right, pl.ds(HALF, HALF)], fa.at[j, pl.ds(HALF, HALF)], fal.at[j], right),
            (part.at[j, left, pl.ds(0, HALF)], fb.at[j, pl.ds(0, HALF)], fbl.at[j], left),
            (part.at[j, right, pl.ds(0, HALF)], fa.at[j, pl.ds(0, HALF)], fal.at[j], right),
            (part.at[j, left, pl.ds(HALF, HALF)], fb.at[j, pl.ds(HALF, HALF)], fbl.at[j], left),
        )

    def rs_start(j):
        for src, dst, sem, to in rs_pieces(j)[:4]:
            remote(src, dst, rs_send_sem, sem, g, to).start()

    def rs_middle(j):
        pieces = rs_pieces(j)
        landed(ha.at[j], hal.at[j])
        part[j, right, 0:HALF, :] = (part[j, right, 0:HALF, :].astype(F32) + ha[j].astype(F32)).astype(BF16)
        src, dst, sem, to = pieces[4]
        remote(src, dst, rs_send_sem, sem, g, to).start()
        landed(hb.at[j], hbl.at[j])
        part[j, left, HALF:CROWS, :] = (part[j, left, HALF:CROWS, :].astype(F32) + hb[j].astype(F32)).astype(BF16)
        src, dst, sem, to = pieces[5]
        remote(src, dst, rs_send_sem, sem, g, to).start()

    def rs_total(j):
        landed(fa.at[j], fal.at[j])
        landed(fb.at[j], fbl.at[j])
        return (part[j, y].astype(F32) + fa[j].astype(F32) + fb[j].astype(F32)).astype(BF16)

    def project(c):
        col = pl.multiple_of(c * BLK, BLK)

        def quarter(q, carry):
            r = pl.multiple_of(q * QROWS, QROWS)
            part[c, q] = jnp.dot(act[pl.ds(r, QROWS), :], proj[:, pl.ds(col, BLK)], preferred_element_type=F32).astype(BF16)
            return carry

        lax.fori_loop(0, TP, quarter, 0)
        rs_start(c)

    def conv_end(c):
        col = pl.multiple_of(c * BLK, BLK)
        cov[:, pl.ds(col, BLK)] = rs_total(c)
        pltpu.make_async_copy(cov.at[:, pl.ds(col, BLK)], co_hbm.at[:, pl.ds(col, BLK)], put_sem.at[0]).start()

    def crows(c):
        return pl.ds(pl.multiple_of(c * CROWS, CROWS), CROWS)

    def hrows(c, h):
        return pl.ds(pl.multiple_of(c * CROWS + h * HALF, HALF), HALF)

    def colof(t):
        return pl.ds(pl.multiple_of(t * BLK, BLK), BLK)

    def gather_start(c):
        @pl.when(c == NCH - 1)
        def _():
            landed(xg.at[pl.ds(0, CROWS - CAP), pl.ds(0, BLK)], dsp_recv.at[c])

        @pl.when(c < NCH - 1)
        def _():
            landed(xg.at[pl.ds(0, CROWS), pl.ds(0, BLK)], dsp_recv.at[c])

        block = xg.at[crows(c), colof(y)]
        remote(block, block, ag_send, agl.at[c], g, right).start()
        remote(block, block, ag_send, agr.at[c], g, left).start()

    def gather_forward(c):
        landed(xg.at[crows(c), colof(left)], agl.at[c])
        piece = xg.at[hrows(c, 0), colof(left)]
        remote(piece, piece, ag_send, agfl.at[c], g, right).start()
        landed(xg.at[crows(c), colof(right)], agr.at[c])
        piece = xg.at[hrows(c, 1), colof(right)]
        remote(piece, piece, ag_send, agfr.at[c], g, left).start()

    def experts(c):
        landed(xg.at[hrows(c, 0), colof(opp)], agfl.at[c])
        landed(xg.at[hrows(c, 1), colof(opp)], agfr.at[c])

        def up(n, carry):
            cols = pl.ds(pl.multiple_of(n * 256, 256), 256)
            rows = xg[crows(c), :]
            gate = jnp.dot(rows, wg[:, cols], preferred_element_type=F32)
            value = jnp.dot(rows, wu[:, cols], preferred_element_type=F32)
            hid[:, cols] = (gate / (1.0 + jnp.exp(-gate)) * value).astype(BF16)
            return carry

        lax.fori_loop(0, BLK // 256, up, 0)

        def down(q, carry):
            part[NCH + c, q] = jnp.dot(hid[...], wd[:, colof(q)], preferred_element_type=F32).astype(BF16)
            return carry

        lax.fori_loop(0, TP, down, 0)
        rs_start(NCH + c)

    def give_back(c):
        rout[crows(c), :] = rs_total(NCH + c)

        def one(j, carry):
            i = c * CSRC + j

            @pl.when(i != OWN)
            def _():
                remote(
                    rout.at[pl.ds(pl.multiple_of(i * CAP, CAP), CAP), :],
                    rin.at[pl.ds(pl.multiple_of(g * CAP, CAP), CAP), :],
                    ret_send,
                    ret_recv,
                    behind(i),
                    y,
                ).start()

            return carry

        lax.fori_loop(0, CSRC, one, 0)

        @pl.when(c == NCH - 1)
        def _():
            rin[pl.ds(pl.multiple_of(g * CAP, CAP), CAP), :] = rout[OWN * CAP : OWN * CAP + CAP, :]

    project(0)
    for load in loads[3:]:
        load.wait()

    def step(k, carry):
        @pl.when((k >= 1) & (k <= NCH))
        def _():
            gather_forward(k - 1)

        @pl.when(k < NCH)
        def _():
            gather_start(k)

        @pl.when((k >= 2) & (k <= NCH + 1))
        def _():
            rs_middle(NCH + k - 2)

        @pl.when((k <= 1) | (k == NCH + 1))
        def _():
            rs_middle(k - 3 * (k // 5))

        @pl.when((k >= 1) & (k <= NCH))
        def _():
            experts(k - 1)

        @pl.when((k == 0) | (k >= NCH))
        def _():
            project(1 + (k + 1) // 5 + k // 5)

        @pl.when((k >= 2) & (k <= NCH + 1))
        def _():
            give_back(k - 2)

        @pl.when((k <= 1) | (k == NCH + 1))
        def _():
            conv_end(k - 3 * (k // 5))

        return carry

    lax.fori_loop(0, NCH + 2, step, 0)
    rs_middle(3)

    landed(rin.at[pl.ds(0, SLOTS - CAP), :], ret_recv)
    combined = jnp.dot(whi[...], rin[...], preferred_element_type=F32)
    combined = combined + jnp.dot(wlo[...], rin[...], preferred_element_type=F32)
    cmb[...] = combined.astype(BF16)
    for d in range(1, TP):
        to = (y + d) % TP
        sends.append(
            remote(
                cmb.at[pl.ds(pl.multiple_of(to * TOK, TOK), TOK), :],
                mo.at[:, pl.ds(ycol, BLK)],
                fin_send.at[d],
                fin_recv.at[d],
                g,
                to,
            )
        )
        sends[-1].start()
    mo[:, pl.ds(ycol, BLK)] = cmb[pl.ds(pl.multiple_of(y * TOK, TOK), TOK), :]

    conv_end(3)
    for d in range(1, TP):
        landed(mo.at[:, pl.ds(0, BLK)], fin_recv.at[d])
    out = pltpu.make_async_copy(mo, mo_hbm, put_sem.at[1])
    out.start()

    for send in sends + stat_sends:
        send.wait_send()

    @pl.when(g < EP - 1)
    def _():
        halo.wait_send()

    landed(dsp.at[pl.ds(0, SLOTS - CAP), :], dsp_send)
    landed(rout.at[pl.ds(0, SLOTS - CAP), :], ret_send)
    landed(xg.at[pl.ds(0, 3 * CROWS), :], ag_send)
    landed(part.at[:, pl.ds(0, 3)], rs_send_sem)
    landed(cov, put_sem.at[0])
    out.wait()


def local(
    conv_input, conv_kernel, norm_gain, norm_shift, conv_proj, moe_input, moe_gain, routes, route_weights,
    gate_proj, up_proj, down_proj,
):
    vmem = pl.BlockSpec(memory_space=pltpu.VMEM)
    hbm = pl.BlockSpec(memory_space=pl.ANY)
    dma, jobs = pltpu.SemaphoreType.DMA, 2 * NCH
    v = pltpu.VMEM
    return pl.pallas_call(
        kernel,
        out_shape=(
            jax.ShapeDtypeStruct((QROWS, D), BF16),
            jax.ShapeDtypeStruct((TOK, D), BF16),
        ),
        in_specs=[hbm, vmem, vmem, vmem, hbm, hbm, vmem, vmem, vmem, hbm, hbm, hbm],
        out_specs=(hbm, hbm),
        scratch_shapes=[
            v((HALO + ROWS, BLK), BF16),
            v((NCB, HALO + ROWS, 128), F32),
            v((NCB, 32, 128), F32),
            v((NCB, ROWS, 128), F32),
            v((TP + 1, RB, 128), F32),
            v((ROWS, BLK), BF16),
            v((BLK, D), BF16),
            v((TOK, D), BF16),
            v((D, BLK), BF16),
            v((D, BLK), BF16),
            v((BLK, D), BF16),
            v((TOK, D), BF16),
            v((GROUP, BLK), BF16),
            v((SLOTS, BLK), BF16),
            v((SLOTS, D), BF16),
            v((CROWS, BLK), BF16),
            v((jobs, TP, CROWS, BLK), BF16),
            v((jobs, HALF, BLK), BF16),
            v((jobs, HALF, BLK), BF16),
            v((jobs, CROWS, BLK), BF16),
            v((jobs, CROWS, BLK), BF16),
            v((SLOTS, BLK), BF16),
            v((SLOTS, BLK), BF16),
            v((GROUP, SLOTS), BF16),
            v((GROUP, SLOTS), BF16),
            v((GROUP, BLK), BF16),
            v((TOK, D), BF16),
            v((QROWS, D), BF16),
            dma((6,)),
            dma((2,)),
            dma((2,)),
            dma((TP,)),
            dma((TP,)),
            dma((TP,)),
            dma((TP,)),
            dma,
            dma((NCH,)),
            dma,
            dma((NCH,)),
            dma((NCH,)),
            dma((NCH,)),
            dma((NCH,)),
            dma,
            dma((jobs,)),
            dma((jobs,)),
            dma((jobs,)),
            dma((jobs,)),
            dma,
            dma,
            dma((TP,)),
            dma((TP,)),
        ],
        compiler_params=pltpu.CompilerParams(
            collective_id=0, has_side_effects=True, vmem_limit_bytes=60 * 1024 * 1024
        ),
    )(
        conv_input,
        conv_kernel,
        norm_gain.reshape(1, BLK),
        norm_shift.reshape(1, BLK),
        conv_proj,
        moe_input,
        moe_gain.reshape(1, D),
        routes.T,
        route_weights.T,
        gate_proj,
        up_proj,
        down_proj,
    )


def solution(mesh):
    placed = (
        P("ep", "tp"),
        P(None, "tp"),
        P("tp"),
        P("tp"),
        P("tp", None),
        P(("ep", "tp"), None),
        P(),
        P("ep", None),
        P("ep", None),
        P("ep", None, "tp"),
        P("ep", None, "tp"),
        P("ep", "tp", None),
    )
    return jax.shard_map(
        local,
        mesh=mesh,
        in_specs=placed,
        out_specs=(P(("ep", "tp"), None), P(("ep", "tp"), None)),
        check_vma=False,
    )
```

```python
import jax
import jax.numpy as jnp
from jax import lax
from jax.experimental import pallas as pl
from jax.experimental.pallas import tpu as pltpu
from jax.sharding import PartitionSpec as P

MESH = pl.DeviceIdType.MESH
F32 = jnp.float32
BF16 = jnp.bfloat16

EP = 64
TP = 4
D = 2048
BLK = D // TP
GROUP = 256
TOK = GROUP // TP
CAP = 16
SLOTS = EP * CAP
NCH = 4
CROWS = SLOTS // NCH
CSRC = EP // NCH
HALF = CROWS // 2
ROWS = 1024
QROWS = ROWS // TP
HALO = 32
TAPS = 31
RB = 64
NRB = ROWS // RB
NCB = BLK // 128
PIECE = 64
STEPS_Z = ((1, 6), (3, 4), (2, 5), (0, 7))
OWN = 48


def kernel(
    x_hbm, ck_ref, gain_ref, shift_ref, proj_hbm, mi_hbm, mgain_ref, rt_ref, rw_ref, wg_hbm, wu_hbm, wd_hbm,
    cov, mo,
    xb, xf, ckf, mixed, tst, act, actf, proj, mi, wg, wu, wd, nrm, grp, dsp, xg, hid, part, fa, fb,
    rout, rin, rin2, whi, wlo, cmb, fin,
    load_sem, halo_sem, grp_send, grp_recv, st_send, st_recv, dsp_send, dsp_recv,
    act_send, act_recv, w_send, wy, wxl, wxr, wfl, wfr, wc, ag_send, agl, agr, agfl, agfr, rs_send_sem, fal, fbl, ret_send, ret_recv, ret2_send, ret2_recv, fin_send, fin_recv,
):
    g = lax.axis_index("ep")
    y = lax.axis_index("tp")
    right, left, opp = (y + 1) % TP, (y + 3) % TP, (y + 2) % TP
    z, xx, core = g // 8, (g % 8) // 2, g % 2
    ycol = pl.multiple_of(y * BLK, BLK)

    def offsets(i):
        c, j = i // CSRC, i % CSRC
        return STEPS_Z[c][j % 2], j // 4, (j // 2) % 2

    zbase = [((z + dz) % 8) * 8 for dz in range(8)]
    xbase = [[((xx + dx) % 4) * 2 + (core + dc) % 2 for dc in range(2)] for dx in range(4)]
    others = [i for i in range(EP) if i != OWN]

    def ahead(i):
        dz, dx, dc = offsets(i)
        return zbase[dz] + xbase[dx][dc]

    def behind(i):
        dz, dx, dc = offsets(i)
        return zbase[-dz % 8] + xbase[-dx % 4][dc]

    def remote(src, dst, send, recv, ep, tp):
        return pltpu.make_async_remote_copy(
            src_ref=src, dst_ref=dst, send_sem=send, recv_sem=recv, device_id=(ep, tp), device_id_type=MESH
        )

    def landed(ref, sem):
        pltpu.make_async_copy(ref, ref, sem).wait()

    loads = [
        pltpu.make_async_copy(mi_hbm, mi, load_sem.at[0]),
        pltpu.make_async_copy(x_hbm, xb.at[pl.ds(HALO, ROWS)], load_sem.at[1]),
        pltpu.make_async_copy(proj_hbm, proj.at[pl.ds(ycol, BLK)], load_sem.at[2]),
        pltpu.make_async_copy(wg_hbm.at[0], wg, load_sem.at[3]),
        pltpu.make_async_copy(wu_hbm.at[0], wu, load_sem.at[4]),
        pltpu.make_async_copy(wd_hbm.at[0], wd, load_sem.at[5]),
    ]
    barrier = pltpu.get_barrier_semaphore()
    for d in range(1, TP):
        pl.semaphore_signal(barrier, inc=1, device_id=(g, (y + d) % TP), device_id_type=MESH)

    loads[0].start()
    for i in others:
        pl.semaphore_signal(barrier, inc=1, device_id=(ahead(i), y), device_id_type=MESH)
    for load in loads[1:]:
        load.start()

    loads[0].wait()
    rows = mi[...].astype(F32)
    scale = lax.rsqrt(jnp.mean(rows * rows, axis=1, keepdims=True) + 1e-6)
    nrm[...] = (rows * scale * mgain_ref[...]).astype(BF16)
    grp[pl.ds(pl.multiple_of(y * TOK, TOK), TOK), :] = nrm[:, pl.ds(ycol, BLK)]

    pl.semaphore_wait(barrier, EP - 1 + TP - 1)

    sends = []
    for d in range(1, TP):
        to = (y + d) % TP
        sends.append(
            remote(
                nrm.at[:, pl.ds(pl.multiple_of(to * BLK, BLK), BLK)],
                grp.at[pl.ds(pl.multiple_of(y * TOK, TOK), TOK), :],
                grp_send.at[d],
                grp_recv.at[d],
                g,
                to,
            )
        )
        sends[-1].start()

    xnext, xprev = zbase[0] + xbase[1][0], zbase[0] + xbase[3][0]
    partner = zbase[0] + xbase[0][1]
    shards = [(y + d) % TP for d in range(1, TP)]

    def shard_rows(t, start, count):
        return proj.at[pl.ds(pl.multiple_of(t * BLK + start, PIECE // 2), count)]

    half_at = core * (BLK // 2)
    piece_at = half_at + xx * PIECE
    def share_y():
        loads[2].wait()
        block = shard_rows(y, piece_at, PIECE)
        remote(block, block, w_send, wy.at[0], g, right).start()
        remote(block, block, w_send, wy.at[1], g, left).start()

    def share_yy():
        landed(proj.at[pl.ds(0, PIECE)], wy.at[0])
        block = shard_rows(left, piece_at, PIECE // 2)
        remote(block, block, w_send, wy.at[2], g, right).start()
        landed(proj.at[pl.ds(0, PIECE)], wy.at[1])
        block = shard_rows(right, piece_at + PIECE // 2, PIECE // 2)
        remote(block, block, w_send, wy.at[3], g, left).start()

    def share_x():
        landed(proj.at[pl.ds(0, PIECE // 2)], wy.at[2])
        landed(proj.at[pl.ds(0, PIECE // 2)], wy.at[3])
        for t in shards:
            block = shard_rows(t, piece_at, PIECE)
            remote(block, block, w_send, wxl, xnext, y).start()
            remote(block, block, w_send, wxr, xprev, y).start()

    def share_xx():
        landed(proj.at[pl.ds(0, 3 * PIECE)], wxl)
        landed(proj.at[pl.ds(0, 3 * PIECE)], wxr)
        for t in shards:
            block = shard_rows(t, half_at + ((xx + 3) % 4) * PIECE, PIECE // 2)
            remote(block, block, w_send, wfl, xnext, y).start()
            block = shard_rows(t, half_at + ((xx + 1) % 4) * PIECE + PIECE // 2, PIECE // 2)
            remote(block, block, w_send, wfr, xprev, y).start()

    def share_core():
        landed(proj.at[pl.ds(0, 3 * PIECE // 2)], wfl)
        landed(proj.at[pl.ds(0, 3 * PIECE // 2)], wfr)
        for t in shards:
            block = shard_rows(t, half_at, BLK // 2)
            remote(block, block, w_send, wc, partner, y).start()

    loads[1].wait()
    halo = remote(xb.at[pl.ds(ROWS, HALO)], xb.at[pl.ds(0, HALO)], halo_sem.at[0], halo_sem.at[1], (g + 1) % EP, y)

    @pl.when(g < EP - 1)
    def _():
        halo.start()

    expert_col = lax.broadcasted_iota(jnp.int32, (EP, GROUP), 0)
    named = (rt_ref[0:1, :] == expert_col) | (rt_ref[1:2, :] == expert_col)
    named_f = jnp.where(named, 1.0, 0.0)
    earlier = lax.broadcasted_iota(jnp.int32, (GROUP, GROUP), 0) < lax.broadcasted_iota(jnp.int32, (GROUP, GROUP), 1)
    rank = jnp.dot(named_f.astype(BF16), jnp.where(earlier, 1.0, 0.0).astype(BF16), preferred_element_type=F32)
    rank = jnp.where(named, rank, -1.0).astype(BF16)
    slot = lax.broadcasted_iota(jnp.int32, (SLOTS, EP), 0)
    spread_rows = jnp.where(slot // CAP == lax.broadcasted_iota(jnp.int32, (SLOTS, EP), 1), 1.0, 0.0).astype(BF16)
    ranks = jnp.dot(spread_rows, rank, preferred_element_type=F32)
    place = (lax.broadcasted_iota(jnp.int32, (SLOTS, GROUP), 0) % CAP).astype(F32)
    chosen = jnp.where(ranks == place, 1.0, 0.0).astype(BF16)
    for d in range(1, TP):
        landed(grp.at[pl.ds(0, TOK), :], grp_recv.at[d])
    dsp[...] = jnp.dot(chosen, grp[...], preferred_element_type=F32).astype(BF16)

    def dispatch(c):
        for i in range(c * CSRC, c * CSRC + CSRC):
            if i != OWN:
                e = ahead(i)
                remote(
                    dsp.at[pl.ds(pl.multiple_of(e * CAP, CAP), CAP), :],
                    xg.at[pl.ds(i * CAP, CAP), pl.ds(ycol, BLK)],
                    dsp_send,
                    dsp_recv.at[c],
                    e,
                    y,
                ).start()

    dispatch(0)
    share_y()
    xg[OWN * CAP : OWN * CAP + CAP, pl.ds(ycol, BLK)] = dsp[pl.ds(pl.multiple_of(g * CAP, CAP), CAP), :]

    def return_rows(c, source, start, target, send, recv):
        for i in range(c * CSRC, c * CSRC + CSRC):
            if i != OWN:
                remote(
                    source.at[pl.ds(start + (i - c * CSRC) * CAP, CAP), :],
                    target.at[pl.ds(pl.multiple_of(g * CAP, CAP), CAP), :],
                    send,
                    recv,
                    behind(i),
                    y,
                ).start()

    def rs_total(c):
        landed(fa.at[c], fal.at[c])
        landed(fb.at[c], fbl.at[c])
        return (part[c, y].astype(F32) + fa[c].astype(F32) + fb[c].astype(F32)).astype(BF16)

    def crows(c):
        return pl.ds(c * CROWS, CROWS)

    def hrows(c, h):
        return pl.ds(c * CROWS + h * HALF, HALF)

    def colof(t):
        return pl.ds(pl.multiple_of(t * BLK, BLK), BLK)

    def gather_start(c):
        landed(xg.at[pl.ds(0, CROWS - CAP if c == NCH - 1 else CROWS), pl.ds(0, BLK)], dsp_recv.at[c])
        block = xg.at[crows(c), colof(y)]
        remote(block, block, ag_send, agl.at[c], g, right).start()
        remote(block, block, ag_send, agr.at[c], g, left).start()

    def gather_forward(c):
        landed(xg.at[crows(c), colof(left)], agl.at[c])
        piece = xg.at[hrows(c, 0), colof(left)]
        remote(piece, piece, ag_send, agfl.at[c], g, right).start()
        landed(xg.at[crows(c), colof(right)], agr.at[c])
        piece = xg.at[hrows(c, 1), colof(right)]
        remote(piece, piece, ag_send, agfr.at[c], g, left).start()

    def experts(c):
        landed(xg.at[hrows(c, 0), colof(opp)], agfl.at[c])
        landed(xg.at[hrows(c, 1), colof(opp)], agfr.at[c])

        def up(n, carry):
            cols = pl.ds(pl.multiple_of(n * 256, 256), 256)
            rows = xg[crows(c), :]
            gate = jnp.dot(rows, wg[:, cols], preferred_element_type=F32)
            value = jnp.dot(rows, wu[:, cols], preferred_element_type=F32)
            hid[:, cols] = (gate / (1.0 + jnp.exp(-gate)) * value).astype(BF16)
            return carry

        lax.fori_loop(0, BLK // 256, up, 0)

        def down(q):
            part[c, q] = jnp.dot(hid[...], wd[:, colof(q)], preferred_element_type=F32).astype(BF16)

        down(right)
        remote(part.at[c, right], fa.at[c], rs_send_sem, fal.at[c], g, right).start()
        down(left)
        remote(part.at[c, left], fb.at[c], rs_send_sem, fbl.at[c], g, left).start()
        down(opp)
        return_rows(c, part.at[c, opp], 0, rin2, ret2_send, ret2_recv)
        if c == NCH - 1:
            rin2[pl.ds(pl.multiple_of(g * CAP, CAP), CAP), :] = part[c, opp, 0:CAP, :]
        down(y)

    def give_back(c):
        rout[crows(c), :] = rs_total(c)

        return_rows(c, rout, c * CROWS, rin, ret_send, ret_recv)
        if c == NCH - 1:
            rin[pl.ds(pl.multiple_of(g * CAP, CAP), CAP), :] = rout[OWN * CAP : OWN * CAP + CAP, :]

    def conv_out(first, last):
        def columns(n, carry):
            cols = pl.ds(pl.multiple_of(n * 256, 256), 256)
            cov[:, cols] = jnp.dot(actf[...], proj[:, cols], preferred_element_type=F32).astype(BF16)
            return carry

        lax.fori_loop(first, last, columns, 0)

    for cb in range(NCB):
        ckf[cb, 0:TAPS, :] = ck_ref[:, cb * 128 : cb * 128 + 128].astype(F32)

    def widen(b, carry):
        r = pl.multiple_of(HALO + b * 64, 32)
        for cb in range(NCB):
            xf[cb, pl.ds(r, 64), :] = xb[pl.ds(r, 64), cb * 128 : cb * 128 + 128].astype(F32)
        return carry

    lax.fori_loop(0, ROWS // 64, widen, 0)

    lane = lax.broadcasted_iota(jnp.int32, (RB, 128), 1)

    def conv_rows(rb, stats):
        base = pl.multiple_of(rb * RB, RB)
        total = jnp.zeros((RB, 128), F32)
        squares = jnp.zeros((RB, 128), F32)
        for cb in range(NCB):
            acc = jnp.zeros((RB, 128), F32)
            for tap in range(TAPS):
                acc = acc + xf[cb, pl.ds(base + (2 + tap), RB), :] * ckf[cb, tap : tap + 1, :]
            mixed[cb, pl.ds(base, RB), :] = acc
            total = total + acc
            squares = squares + acc * acc
        stats = jnp.where(lane == rb, jnp.sum(total, axis=1, keepdims=True), stats)
        return jnp.where(lane == rb + NRB, jnp.sum(squares, axis=1, keepdims=True), stats)

    stats = lax.fori_loop(1, NRB // 2, conv_rows, jnp.zeros((RB, 128), F32))
    dispatch(1)
    gather_start(0)
    dispatch(2)
    share_yy()
    @pl.when(g > 0)
    def _():
        halo.wait_recv()

    @pl.when(g == 0)
    def _():
        xb[0:HALO, :] = jnp.zeros((HALO, BLK), BF16)

    for cb in range(NCB):
        xf[cb, 0:HALO, :] = xb[0:HALO, cb * 128 : cb * 128 + 128].astype(F32)
    stats = lax.fori_loop(NRB // 2, NRB, conv_rows, stats)
    stats = conv_rows(0, stats)
    tst[TP] = stats
    stat_sends = []
    for d in range(1, TP):
        to = (y + d) % TP
        stat_sends.append(remote(tst.at[TP], tst.at[y], st_send.at[d], st_recv.at[d], g, to))
        stat_sends[-1].start()

    gather_forward(0)
    gather_start(1)
    dispatch(3)
    pick = lax.broadcasted_iota(jnp.int32, (128, GROUP), 0)
    table = jnp.where(pick == 0, rt_ref[0:1, :].astype(F32), 0.0)
    table = jnp.where(pick == 1, rt_ref[1:2, :].astype(F32), table)
    table = jnp.where(pick == 2, rw_ref[0:1, :], table)
    table = jnp.where(pick == 3, rw_ref[1:2, :], table)
    table = jnp.transpose(table)
    expert_lane = lax.broadcasted_iota(jnp.int32, (GROUP, EP), 1).astype(F32)
    first = table[:, 0:1] == expert_lane
    second = table[:, 1:2] == expert_lane
    named_t = jnp.where(first | second, 1.0, 0.0)
    before = lax.broadcasted_iota(jnp.int32, (GROUP, GROUP), 1) < lax.broadcasted_iota(jnp.int32, (GROUP, GROUP), 0)
    rank_t = jnp.dot(jnp.where(before, 1.0, 0.0).astype(BF16), named_t.astype(BF16), preferred_element_type=F32)
    rank_t = jnp.where(first | second, rank_t, -1.0).astype(BF16)
    weight_t = jnp.where(first, table[:, 2:3], 0.0) + jnp.where(second, table[:, 3:4], 0.0)
    weight_hi = weight_t.astype(BF16)
    weight_lo = (weight_t - weight_hi.astype(F32)).astype(BF16)
    slot_lane = lax.broadcasted_iota(jnp.int32, (EP, SLOTS), 1)
    spread_cols = jnp.where(slot_lane // CAP == lax.broadcasted_iota(jnp.int32, (EP, SLOTS), 0), 1.0, 0.0).astype(BF16)
    hit = jnp.dot(rank_t, spread_cols, preferred_element_type=F32) == (
        lax.broadcasted_iota(jnp.int32, (GROUP, SLOTS), 1) % CAP
    ).astype(F32)
    whi[...] = jnp.where(hit, jnp.dot(weight_hi, spread_cols, preferred_element_type=F32), 0.0).astype(BF16)
    wlo[...] = jnp.where(hit, jnp.dot(weight_lo, spread_cols, preferred_element_type=F32), 0.0).astype(BF16)

    for d in range(1, TP):
        landed(tst.at[0], st_recv.at[d])
    means = (tst[TP] + tst[right] + tst[opp] + tst[left]) * (1.0 / D)

    def activate(rb, carry):
        base = pl.multiple_of(rb * RB, RB)
        center = jnp.sum(jnp.where(lane == rb, means, 0.0), axis=1, keepdims=True)
        square = jnp.sum(jnp.where(lane == rb + NRB, means, 0.0), axis=1, keepdims=True)
        inv = lax.rsqrt(jnp.maximum(square - center * center, 0.0) + 1e-5)
        for cb in range(NCB):
            cols = slice(cb * 128, cb * 128 + 128)
            v = (mixed[cb, pl.ds(base, RB), :] - center) * inv * gain_ref[:, cols] + shift_ref[:, cols]
            act[pl.ds(base, RB), cols] = (v / (1.0 + jnp.exp(-v))).astype(BF16)
        return carry

    lax.fori_loop(0, NRB, activate, 0)
    def share_act(d):
        to = (y + d) % TP
        remote(
            act.at[pl.ds(pl.multiple_of(to * QROWS, QROWS), QROWS)],
            actf.at[:, pl.ds(ycol, BLK)],
            act_send,
            act_recv.at[d],
            g,
            to,
        ).start()

    actf[:, pl.ds(ycol, BLK)] = act[pl.ds(pl.multiple_of(y * QROWS, QROWS), QROWS), :]

    for load in loads[3:]:
        load.wait()
    share_x()
    experts(0)
    gather_forward(1)
    gather_start(2)
    give_back(0)
    experts(1)
    gather_forward(2)
    gather_start(3)
    give_back(1)
    experts(2)
    share_xx()
    gather_forward(3)
    give_back(2)
    experts(3)
    share_core()
    give_back(3)
    share_act(2)
    share_act(1)
    share_act(3)

    def combine(rows):
        total = jnp.dot(whi[...], rows[...], preferred_element_type=F32)
        return (total + jnp.dot(wlo[...], rows[...], preferred_element_type=F32)).astype(BF16)

    def to_owners(half):
        for d in (2, 1, 3):
            to = (y + d) % TP
            sends.append(
                remote(
                    cmb.at[half, pl.ds(pl.multiple_of(to * TOK, TOK), TOK), :],
                    fin.at[half, y],
                    fin_send.at[d + 4 * half],
                    fin_recv.at[d + 4 * half],
                    g,
                    to,
                )
            )
            sends[-1].start()
        fin[half, y] = cmb[half, pl.ds(pl.multiple_of(y * TOK, TOK), TOK), :]

    landed(rin2.at[pl.ds(0, SLOTS - CAP), :], ret2_recv)
    cmb[1] = combine(rin2)
    to_owners(1)
    landed(rin.at[pl.ds(0, SLOTS - CAP), :], ret_recv)
    cmb[0] = combine(rin)
    to_owners(0)
    landed(proj.at[pl.ds(0, 3 * (BLK // 2))], wc)
    for d in range(1, TP):
        landed(actf.at[:, pl.ds(0, BLK)], act_recv.at[d])
    conv_out(0, 8)

    for d in range(1, TP):
        landed(fin.at[0, 0], fin_recv.at[d])
        landed(fin.at[0, 0], fin_recv.at[d + 4])
    for t in range(TP):
        both = fin[0, t].astype(F32) + fin[1, (t + 2) % TP].astype(F32)
        mo[:, t * BLK : t * BLK + BLK] = both.astype(BF16)

    for send in sends + stat_sends:
        send.wait_send()

    @pl.when(g < EP - 1)
    def _():
        halo.wait_send()

    landed(dsp.at[pl.ds(0, SLOTS - CAP), :], dsp_send)
    landed(rout.at[pl.ds(0, SLOTS - CAP), :], ret_send)
    landed(xg.at[pl.ds(0, 3 * CROWS), :], ag_send)
    landed(part.at[:, pl.ds(0, 2)], rs_send_sem)
    landed(rout.at[pl.ds(0, SLOTS - CAP), :], ret2_send)
    landed(act.at[pl.ds(0, 3 * QROWS)], act_send)
    landed(proj.at[pl.ds(0, 24 * PIECE)], w_send)


def local(
    conv_input, conv_kernel, norm_gain, norm_shift, conv_proj, moe_input, moe_gain, routes, route_weights,
    gate_proj, up_proj, down_proj,
):
    vmem = pl.BlockSpec(memory_space=pltpu.VMEM)
    hbm = pl.BlockSpec(memory_space=pl.ANY)
    dma, jobs = pltpu.SemaphoreType.DMA, NCH
    v = pltpu.VMEM
    return pl.pallas_call(
        kernel,
        out_shape=(
            pltpu.VMEM((QROWS, D), BF16),
            pltpu.VMEM((TOK, D), BF16),
        ),
        in_specs=[hbm, vmem, vmem, vmem, hbm, hbm, vmem, vmem, vmem, hbm, hbm, hbm],
        out_specs=(vmem, vmem),
        scratch_shapes=[
            v((HALO + ROWS, BLK), BF16),
            v((NCB, HALO + ROWS, 128), F32),
            v((NCB, 32, 128), F32),
            v((NCB, ROWS, 128), F32),
            v((TP + 1, RB, 128), F32),
            v((ROWS, BLK), BF16),
            v((QROWS, D), BF16),
            v((D, D), BF16),
            v((TOK, D), BF16),
            v((D, BLK), BF16),
            v((D, BLK), BF16),
            v((BLK, D), BF16),
            v((TOK, D), BF16),
            v((GROUP, BLK), BF16),
            v((SLOTS, BLK), BF16),
            v((SLOTS, D), BF16),
            v((CROWS, BLK), BF16),
            v((jobs, TP, CROWS, BLK), BF16),
            v((jobs, CROWS, BLK), BF16),
            v((jobs, CROWS, BLK), BF16),
            v((SLOTS, BLK), BF16),
            v((SLOTS, BLK), BF16),
            v((SLOTS, BLK), BF16),
            v((GROUP, SLOTS), BF16),
            v((GROUP, SLOTS), BF16),
            v((2, GROUP, BLK), BF16),
            v((2, TP, TOK, BLK), BF16),
            dma((6,)),
            dma((2,)),
            dma((TP,)),
            dma((TP,)),
            dma((TP,)),
            dma((TP,)),
            dma,
            dma((NCH,)),
            dma,
            dma((TP,)),
            dma,
            dma((TP,)),
            dma,
            dma,
            dma,
            dma,
            dma,
            dma,
            dma((NCH,)),
            dma((NCH,)),
            dma((NCH,)),
            dma((NCH,)),
            dma,
            dma((jobs,)),
            dma((jobs,)),
            dma,
            dma,
            dma,
            dma,
            dma((8,)),
            dma((8,)),
        ],
        compiler_params=pltpu.CompilerParams(
            collective_id=0, has_side_effects=True, vmem_limit_bytes=60 * 1024 * 1024
        ),
    )(
        conv_input,
        conv_kernel,
        norm_gain.reshape(1, BLK),
        norm_shift.reshape(1, BLK),
        conv_proj,
        moe_input,
        moe_gain.reshape(1, D),
        routes.T,
        route_weights.T,
        gate_proj,
        up_proj,
        down_proj,
    )


def solution(mesh):
    placed = (
        P("ep", "tp"),
        P(None, "tp"),
        P("tp"),
        P("tp"),
        P("tp", None),
        P(("ep", "tp"), None),
        P(),
        P("ep", None),
        P("ep", None),
        P("ep", None, "tp"),
        P("ep", None, "tp"),
        P("ep", "tp", None),
    )
    return jax.shard_map(
        local,
        mesh=mesh,
        in_specs=placed,
        out_specs=(P(("ep", "tp"), None), P(("ep", "tp"), None)),
        check_vma=False,
    )
```

```python
import jax
import jax.numpy as jnp
from jax import lax
from jax.experimental import pallas as pl
from jax.experimental.pallas import tpu as pltpu
from jax.sharding import PartitionSpec as P

MESH = pl.DeviceIdType.MESH
F32 = jnp.float32
BF16 = jnp.bfloat16

EP = 64
TP = 4
D = 2048
BLK = D // TP
GROUP = 256
TOK = GROUP // TP
CAP = 16
SLOTS = EP * CAP
NCH = 8
CROWS = SLOTS // NCH
CSRC = EP // NCH
HALF = CROWS // 2
ROWS = 1024
QROWS = ROWS // TP
HALO = 32
TAPS = 31
RB = 64
NRB = ROWS // RB
NCB = BLK // 128
PIECE = 64
STEPS_Z = (1, 6, 3, 5, 4, 2, 7, 0)
OWN = 56


def kernel(
    x_hbm, ck_ref, gain_ref, shift_ref, proj_hbm, mi_hbm, mgain_ref, rt_ref, rw_ref, wg_hbm, wu_hbm, wd_hbm,
    cov, mo,
    xb, xf, ckf, mixed, tst, act, actf, proj, mi, wg, wu, wd, nrm, grp, dsp, xg, hid, part, fa, fb,
    rout, rin, rin2, whi, wlo, cmb, fin,
    load_sem, halo_sem, grp_send, grp_recv, st_send, st_recv, dsp_send, dsp_recv,
    act_send, act_recv, w_send, wy, wxl, wxr, wfl, wfr, wc, ag_send, agl, agr, agfl, agfr, rs_send_sem, fal, fbl, ret_send, ret_recv, ret2_send, ret2_recv, fin_send, fin_recv,
):
    g = lax.axis_index("ep")
    y = lax.axis_index("tp")
    right, left, opp = (y + 1) % TP, (y + 3) % TP, (y + 2) % TP
    z, xx, core = g // 8, (g % 8) // 2, g % 2
    ycol = pl.multiple_of(y * BLK, BLK)

    def offsets(i):
        c, j = i // CSRC, i % CSRC
        return STEPS_Z[c], j // 2, j % 2

    zbase = [((z + dz) % 8) * 8 for dz in range(8)]
    xbase = [[((xx + dx) % 4) * 2 + (core + dc) % 2 for dc in range(2)] for dx in range(4)]
    others = [i for i in range(EP) if i != OWN]

    def ahead(i):
        dz, dx, dc = offsets(i)
        return zbase[dz] + xbase[dx][dc]

    def behind(i):
        dz, dx, dc = offsets(i)
        return zbase[-dz % 8] + xbase[-dx % 4][dc]

    def remote(src, dst, send, recv, ep, tp):
        return pltpu.make_async_remote_copy(
            src_ref=src, dst_ref=dst, send_sem=send, recv_sem=recv, device_id=(ep, tp), device_id_type=MESH
        )

    def landed(ref, sem):
        pltpu.make_async_copy(ref, ref, sem).wait()

    loads = [
        pltpu.make_async_copy(mi_hbm, mi, load_sem.at[0]),
        pltpu.make_async_copy(x_hbm, xb.at[pl.ds(HALO, ROWS)], load_sem.at[1]),
        pltpu.make_async_copy(proj_hbm, proj.at[pl.ds(ycol, BLK)], load_sem.at[2]),
        pltpu.make_async_copy(wg_hbm.at[0], wg, load_sem.at[3]),
        pltpu.make_async_copy(wu_hbm.at[0], wu, load_sem.at[4]),
        pltpu.make_async_copy(wd_hbm.at[0], wd, load_sem.at[5]),
    ]
    barrier = pltpu.get_barrier_semaphore()
    for d in range(1, TP):
        pl.semaphore_signal(barrier, inc=1, device_id=(g, (y + d) % TP), device_id_type=MESH)

    loads[0].start()
    for i in others:
        pl.semaphore_signal(barrier, inc=1, device_id=(ahead(i), y), device_id_type=MESH)
    for load in loads[1:]:
        load.start()

    loads[0].wait()
    rows = mi[...].astype(F32)
    scale = lax.rsqrt(jnp.mean(rows * rows, axis=1, keepdims=True) + 1e-6)
    nrm[...] = (rows * scale * mgain_ref[...]).astype(BF16)
    grp[pl.ds(pl.multiple_of(y * TOK, TOK), TOK), :] = nrm[:, pl.ds(ycol, BLK)]

    pl.semaphore_wait(barrier, EP - 1 + TP - 1)

    sends = []
    for d in range(1, TP):
        to = (y + d) % TP
        sends.append(
            remote(
                nrm.at[:, pl.ds(pl.multiple_of(to * BLK, BLK), BLK)],
                grp.at[pl.ds(pl.multiple_of(y * TOK, TOK), TOK), :],
                grp_send.at[d],
                grp_recv.at[d],
                g,
                to,
            )
        )
        sends[-1].start()

    xnext, xprev = zbase[0] + xbase[1][0], zbase[0] + xbase[3][0]
    partner = zbase[0] + xbase[0][1]
    shards = [(y + d) % TP for d in range(1, TP)]

    def shard_rows(t, start, count):
        return proj.at[pl.ds(pl.multiple_of(t * BLK + start, PIECE // 2), count)]

    half_at = core * (BLK // 2)
    piece_at = half_at + xx * PIECE
    def share_y():
        loads[2].wait()
        block = shard_rows(y, piece_at, PIECE)
        remote(block, block, w_send, wy.at[0], g, right).start()
        remote(block, block, w_send, wy.at[1], g, left).start()

    def share_yy():
        landed(proj.at[pl.ds(0, PIECE)], wy.at[0])
        block = shard_rows(left, piece_at, PIECE // 2)
        remote(block, block, w_send, wy.at[2], g, right).start()
        landed(proj.at[pl.ds(0, PIECE)], wy.at[1])
        block = shard_rows(right, piece_at + PIECE // 2, PIECE // 2)
        remote(block, block, w_send, wy.at[3], g, left).start()

    def share_x():
        landed(proj.at[pl.ds(0, PIECE // 2)], wy.at[2])
        landed(proj.at[pl.ds(0, PIECE // 2)], wy.at[3])
        for t in shards:
            block = shard_rows(t, piece_at, PIECE)
            remote(block, block, w_send, wxl, xnext, y).start()
            remote(block, block, w_send, wxr, xprev, y).start()

    def share_xx():
        landed(proj.at[pl.ds(0, 3 * PIECE)], wxl)
        landed(proj.at[pl.ds(0, 3 * PIECE)], wxr)
        for t in shards:
            block = shard_rows(t, half_at + ((xx + 3) % 4) * PIECE, PIECE // 2)
            remote(block, block, w_send, wfl, xnext, y).start()
            block = shard_rows(t, half_at + ((xx + 1) % 4) * PIECE + PIECE // 2, PIECE // 2)
            remote(block, block, w_send, wfr, xprev, y).start()

    def share_core():
        landed(proj.at[pl.ds(0, 3 * PIECE // 2)], wfl)
        landed(proj.at[pl.ds(0, 3 * PIECE // 2)], wfr)
        for t in shards:
            block = shard_rows(t, half_at, BLK // 2)
            remote(block, block, w_send, wc, partner, y).start()

    loads[1].wait()
    halo = remote(xb.at[pl.ds(ROWS, HALO)], xb.at[pl.ds(0, HALO)], halo_sem.at[0], halo_sem.at[1], (g + 1) % EP, y)

    @pl.when(g < EP - 1)
    def _():
        halo.start()

    expert_col = lax.broadcasted_iota(jnp.int32, (EP, GROUP), 0)
    named = (rt_ref[0:1, :] == expert_col) | (rt_ref[1:2, :] == expert_col)
    named_f = jnp.where(named, 1.0, 0.0)
    earlier = lax.broadcasted_iota(jnp.int32, (GROUP, GROUP), 0) < lax.broadcasted_iota(jnp.int32, (GROUP, GROUP), 1)
    rank = jnp.dot(named_f.astype(BF16), jnp.where(earlier, 1.0, 0.0).astype(BF16), preferred_element_type=F32)
    rank = jnp.where(named, rank, -1.0).astype(BF16)
    slot = lax.broadcasted_iota(jnp.int32, (SLOTS, EP), 0)
    spread_rows = jnp.where(slot // CAP == lax.broadcasted_iota(jnp.int32, (SLOTS, EP), 1), 1.0, 0.0).astype(BF16)
    ranks = jnp.dot(spread_rows, rank, preferred_element_type=F32)
    place = (lax.broadcasted_iota(jnp.int32, (SLOTS, GROUP), 0) % CAP).astype(F32)
    chosen = jnp.where(ranks == place, 1.0, 0.0).astype(BF16)
    for d in range(1, TP):
        landed(grp.at[pl.ds(0, TOK), :], grp_recv.at[d])
    dsp[...] = jnp.dot(chosen, grp[...], preferred_element_type=F32).astype(BF16)

    def dispatch(c):
        for i in range(c * CSRC, c * CSRC + CSRC):
            if i != OWN:
                e = ahead(i)
                remote(
                    dsp.at[pl.ds(pl.multiple_of(e * CAP, CAP), CAP), :],
                    xg.at[pl.ds(i * CAP, CAP), pl.ds(ycol, BLK)],
                    dsp_send,
                    dsp_recv.at[c],
                    e,
                    y,
                ).start()

    dispatch(0)
    dispatch(1)
    share_y()
    xg[OWN * CAP : OWN * CAP + CAP, pl.ds(ycol, BLK)] = dsp[pl.ds(pl.multiple_of(g * CAP, CAP), CAP), :]

    def return_rows(c, source, start, target, send, recv):
        for i in range(c * CSRC, c * CSRC + CSRC):
            if i != OWN:
                remote(
                    source.at[pl.ds(start + (i - c * CSRC) * CAP, CAP), :],
                    target.at[pl.ds(pl.multiple_of(g * CAP, CAP), CAP), :],
                    send,
                    recv,
                    behind(i),
                    y,
                ).start()

    def rs_total(c):
        landed(fa.at[c], fal.at[c])
        landed(fb.at[c], fbl.at[c])
        return (part[c, y].astype(F32) + fa[c].astype(F32) + fb[c].astype(F32)).astype(BF16)

    def crows(c):
        return pl.ds(c * CROWS, CROWS)

    def hrows(c, h):
        return pl.ds(c * CROWS + h * HALF, HALF)

    def colof(t):
        return pl.ds(pl.multiple_of(t * BLK, BLK), BLK)

    def gather_start(c):
        landed(xg.at[pl.ds(0, CROWS - CAP if c == OWN // CSRC else CROWS), pl.ds(0, BLK)], dsp_recv.at[c])
        block = xg.at[crows(c), colof(y)]
        remote(block, block, ag_send, agl.at[c], g, right).start()
        remote(block, block, ag_send, agr.at[c], g, left).start()

    def gather_forward(c):
        landed(xg.at[crows(c), colof(left)], agl.at[c])
        piece = xg.at[hrows(c, 0), colof(left)]
        remote(piece, piece, ag_send, agfl.at[c], g, right).start()
        landed(xg.at[crows(c), colof(right)], agr.at[c])
        piece = xg.at[hrows(c, 1), colof(right)]
        remote(piece, piece, ag_send, agfr.at[c], g, left).start()

    def experts(c):
        landed(xg.at[hrows(c, 0), colof(opp)], agfl.at[c])
        landed(xg.at[hrows(c, 1), colof(opp)], agfr.at[c])

        def up(n, carry):
            cols = pl.ds(pl.multiple_of(n * 256, 256), 256)
            rows = xg[crows(c), :]
            gate = jnp.dot(rows, wg[:, cols], preferred_element_type=F32)
            value = jnp.dot(rows, wu[:, cols], preferred_element_type=F32)
            hid[:, cols] = (gate / (1.0 + jnp.exp(-gate)) * value).astype(BF16)
            return carry

        lax.fori_loop(0, BLK // 256, up, 0)

        def down(q):
            part[c, q] = jnp.dot(hid[...], wd[:, colof(q)], preferred_element_type=F32).astype(BF16)

        down(right)
        remote(part.at[c, right], fa.at[c], rs_send_sem, fal.at[c], g, right).start()
        down(left)
        remote(part.at[c, left], fb.at[c], rs_send_sem, fbl.at[c], g, left).start()
        down(opp)
        return_rows(c, part.at[c, opp], 0, rin2, ret2_send, ret2_recv)
        if c == OWN // CSRC:
            rin2[pl.ds(pl.multiple_of(g * CAP, CAP), CAP), :] = part[c, opp, 0:CAP, :]
        down(y)

    def give_back(c):
        rout[crows(c), :] = rs_total(c)

        return_rows(c, rout, c * CROWS, rin, ret_send, ret_recv)
        if c == OWN // CSRC:
            rin[pl.ds(pl.multiple_of(g * CAP, CAP), CAP), :] = rout[OWN * CAP : OWN * CAP + CAP, :]

    def conv_out(first, last):
        def columns(n, carry):
            cols = pl.ds(pl.multiple_of(n * 256, 256), 256)
            cov[:, cols] = jnp.dot(actf[...], proj[:, cols], preferred_element_type=F32).astype(BF16)
            return carry

        lax.fori_loop(first, last, columns, 0)

    for cb in range(NCB):
        ckf[cb, 0:TAPS, :] = ck_ref[:, cb * 128 : cb * 128 + 128].astype(F32)

    def widen(b, carry):
        r = pl.multiple_of(HALO + b * 64, 32)
        for cb in range(NCB):
            xf[cb, pl.ds(r, 64), :] = xb[pl.ds(r, 64), cb * 128 : cb * 128 + 128].astype(F32)
        return carry

    lax.fori_loop(0, ROWS // 64, widen, 0)

    lane = lax.broadcasted_iota(jnp.int32, (RB, 128), 1)

    def conv_rows(rb, stats):
        base = pl.multiple_of(rb * RB, RB)
        total = jnp.zeros((RB, 128), F32)
        squares = jnp.zeros((RB, 128), F32)
        for cb in range(NCB):
            acc = jnp.zeros((RB, 128), F32)
            for tap in range(TAPS):
                acc = acc + xf[cb, pl.ds(base + (2 + tap), RB), :] * ckf[cb, tap : tap + 1, :]
            mixed[cb, pl.ds(base, RB), :] = acc
            total = total + acc
            squares = squares + acc * acc
        stats = jnp.where(lane == rb, jnp.sum(total, axis=1, keepdims=True), stats)
        return jnp.where(lane == rb + NRB, jnp.sum(squares, axis=1, keepdims=True), stats)

    stats = lax.fori_loop(1, NRB // 2, conv_rows, jnp.zeros((RB, 128), F32))
    dispatch(2)
    dispatch(3)
    gather_start(0)
    dispatch(4)
    share_yy()
    @pl.when(g > 0)
    def _():
        halo.wait_recv()

    @pl.when(g == 0)
    def _():
        xb[0:HALO, :] = jnp.zeros((HALO, BLK), BF16)

    for cb in range(NCB):
        xf[cb, 0:HALO, :] = xb[0:HALO, cb * 128 : cb * 128 + 128].astype(F32)
    stats = lax.fori_loop(NRB // 2, NRB, conv_rows, stats)
    stats = conv_rows(0, stats)
    tst[TP] = stats
    stat_sends = []
    for d in range(1, TP):
        to = (y + d) % TP
        stat_sends.append(remote(tst.at[TP], tst.at[y], st_send.at[d], st_recv.at[d], g, to))
        stat_sends[-1].start()

    gather_forward(0)
    gather_start(1)
    dispatch(5)
    dispatch(6)
    dispatch(7)
    pick = lax.broadcasted_iota(jnp.int32, (128, GROUP), 0)
    table = jnp.where(pick == 0, rt_ref[0:1, :].astype(F32), 0.0)
    table = jnp.where(pick == 1, rt_ref[1:2, :].astype(F32), table)
    table = jnp.where(pick == 2, rw_ref[0:1, :], table)
    table = jnp.where(pick == 3, rw_ref[1:2, :], table)
    table = jnp.transpose(table)
    expert_lane = lax.broadcasted_iota(jnp.int32, (GROUP, EP), 1).astype(F32)
    first = table[:, 0:1] == expert_lane
    second = table[:, 1:2] == expert_lane
    named_t = jnp.where(first | second, 1.0, 0.0)
    before = lax.broadcasted_iota(jnp.int32, (GROUP, GROUP), 1) < lax.broadcasted_iota(jnp.int32, (GROUP, GROUP), 0)
    rank_t = jnp.dot(jnp.where(before, 1.0, 0.0).astype(BF16), named_t.astype(BF16), preferred_element_type=F32)
    rank_t = jnp.where(first | second, rank_t, -1.0).astype(BF16)
    weight_t = jnp.where(first, table[:, 2:3], 0.0) + jnp.where(second, table[:, 3:4], 0.0)
    weight_hi = weight_t.astype(BF16)
    weight_lo = (weight_t - weight_hi.astype(F32)).astype(BF16)
    slot_lane = lax.broadcasted_iota(jnp.int32, (EP, SLOTS), 1)
    spread_cols = jnp.where(slot_lane // CAP == lax.broadcasted_iota(jnp.int32, (EP, SLOTS), 0), 1.0, 0.0).astype(BF16)
    hit = jnp.dot(rank_t, spread_cols, preferred_element_type=F32) == (
        lax.broadcasted_iota(jnp.int32, (GROUP, SLOTS), 1) % CAP
    ).astype(F32)
    whi[...] = jnp.where(hit, jnp.dot(weight_hi, spread_cols, preferred_element_type=F32), 0.0).astype(BF16)
    wlo[...] = jnp.where(hit, jnp.dot(weight_lo, spread_cols, preferred_element_type=F32), 0.0).astype(BF16)

    for d in range(1, TP):
        landed(tst.at[0], st_recv.at[d])
    means = (tst[TP] + tst[right] + tst[opp] + tst[left]) * (1.0 / D)

    def activate(rb, carry):
        base = pl.multiple_of(rb * RB, RB)
        center = jnp.sum(jnp.where(lane == rb, means, 0.0), axis=1, keepdims=True)
        square = jnp.sum(jnp.where(lane == rb + NRB, means, 0.0), axis=1, keepdims=True)
        inv = lax.rsqrt(jnp.maximum(square - center * center, 0.0) + 1e-5)
        for cb in range(NCB):
            cols = slice(cb * 128, cb * 128 + 128)
            v = (mixed[cb, pl.ds(base, RB), :] - center) * inv * gain_ref[:, cols] + shift_ref[:, cols]
            act[pl.ds(base, RB), cols] = (v / (1.0 + jnp.exp(-v))).astype(BF16)
        return carry

    lax.fori_loop(0, NRB, activate, 0)
    def share_act(d):
        to = (y + d) % TP
        remote(
            act.at[pl.ds(pl.multiple_of(to * QROWS, QROWS), QROWS)],
            actf.at[:, pl.ds(ycol, BLK)],
            act_send,
            act_recv.at[d],
            g,
            to,
        ).start()

    actf[:, pl.ds(ycol, BLK)] = act[pl.ds(pl.multiple_of(y * QROWS, QROWS), QROWS), :]

    for load in loads[3:]:
        load.wait()
    share_x()
    for k in range(NCH):
        experts(k)
        if k + 1 < NCH:
            gather_forward(k + 1)
        if k + 2 < NCH:
            gather_start(k + 2)
        if k >= 1:
            give_back(k - 1)
        if k == NCH - 3:
            share_xx()
        if k == NCH - 1:
            share_core()
    give_back(NCH - 1)
    share_act(2)
    share_act(1)
    share_act(3)

    def combine(rows):
        total = jnp.dot(whi[...], rows[...], preferred_element_type=F32)
        return (total + jnp.dot(wlo[...], rows[...], preferred_element_type=F32)).astype(BF16)

    def to_owners(half):
        for d in (2, 1, 3):
            to = (y + d) % TP
            sends.append(
                remote(
                    cmb.at[half, pl.ds(pl.multiple_of(to * TOK, TOK), TOK), :],
                    fin.at[half, y],
                    fin_send.at[d + 4 * half],
                    fin_recv.at[d + 4 * half],
                    g,
                    to,
                )
            )
            sends[-1].start()
        fin[half, y] = cmb[half, pl.ds(pl.multiple_of(y * TOK, TOK), TOK), :]

    landed(rin2.at[pl.ds(0, SLOTS - CAP), :], ret2_recv)
    cmb[1] = combine(rin2)
    to_owners(1)
    landed(rin.at[pl.ds(0, SLOTS - CAP), :], ret_recv)
    cmb[0] = combine(rin)
    to_owners(0)
    landed(proj.at[pl.ds(0, 3 * (BLK // 2))], wc)
    for d in range(1, TP):
        landed(actf.at[:, pl.ds(0, BLK)], act_recv.at[d])
    conv_out(0, 8)

    for d in range(1, TP):
        landed(fin.at[0, 0], fin_recv.at[d])
        landed(fin.at[0, 0], fin_recv.at[d + 4])
    for t in range(TP):
        both = fin[0, t].astype(F32) + fin[1, (t + 2) % TP].astype(F32)
        mo[:, t * BLK : t * BLK + BLK] = both.astype(BF16)

    for send in sends + stat_sends:
        send.wait_send()

    @pl.when(g < EP - 1)
    def _():
        halo.wait_send()

    landed(dsp.at[pl.ds(0, SLOTS - CAP), :], dsp_send)
    landed(rout.at[pl.ds(0, SLOTS - CAP), :], ret_send)
    landed(xg.at[pl.ds(0, 3 * SLOTS // TP), :], ag_send)
    landed(part.at[:, pl.ds(0, 2)], rs_send_sem)
    landed(rout.at[pl.ds(0, SLOTS - CAP), :], ret2_send)
    landed(act.at[pl.ds(0, 3 * QROWS)], act_send)
    landed(proj.at[pl.ds(0, 24 * PIECE)], w_send)


def local(
    conv_input, conv_kernel, norm_gain, norm_shift, conv_proj, moe_input, moe_gain, routes, route_weights,
    gate_proj, up_proj, down_proj,
):
    vmem = pl.BlockSpec(memory_space=pltpu.VMEM)
    hbm = pl.BlockSpec(memory_space=pl.ANY)
    dma, jobs = pltpu.SemaphoreType.DMA, NCH
    v = pltpu.VMEM
    return pl.pallas_call(
        kernel,
        out_shape=(
            pltpu.VMEM((QROWS, D), BF16),
            pltpu.VMEM((TOK, D), BF16),
        ),
        in_specs=[hbm, vmem, vmem, vmem, hbm, hbm, vmem, vmem, vmem, hbm, hbm, hbm],
        out_specs=(vmem, vmem),
        scratch_shapes=[
            v((HALO + ROWS, BLK), BF16),
            v((NCB, HALO + ROWS, 128), F32),
            v((NCB, 32, 128), F32),
            v((NCB, ROWS, 128), F32),
            v((TP + 1, RB, 128), F32),
            v((ROWS, BLK), BF16),
            v((QROWS, D), BF16),
            v((D, D), BF16),
            v((TOK, D), BF16),
            v((D, BLK), BF16),
            v((D, BLK), BF16),
            v((BLK, D), BF16),
            v((TOK, D), BF16),
            v((GROUP, BLK), BF16),
            v((SLOTS, BLK), BF16),
            v((SLOTS, D), BF16),
            v((CROWS, BLK), BF16),
            v((jobs, TP, CROWS, BLK), BF16),
            v((jobs, CROWS, BLK), BF16),
            v((jobs, CROWS, BLK), BF16),
            v((SLOTS, BLK), BF16),
            v((SLOTS, BLK), BF16),
            v((SLOTS, BLK), BF16),
            v((GROUP, SLOTS), BF16),
            v((GROUP, SLOTS), BF16),
            v((2, GROUP, BLK), BF16),
            v((2, TP, TOK, BLK), BF16),
            dma((6,)),
            dma((2,)),
            dma((TP,)),
            dma((TP,)),
            dma((TP,)),
            dma((TP,)),
            dma,
            dma((NCH,)),
            dma,
            dma((TP,)),
            dma,
            dma((TP,)),
            dma,
            dma,
            dma,
            dma,
            dma,
            dma,
            dma((NCH,)),
            dma((NCH,)),
            dma((NCH,)),
            dma((NCH,)),
            dma,
            dma((jobs,)),
            dma((jobs,)),
            dma,
            dma,
            dma,
            dma,
            dma((8,)),
            dma((8,)),
        ],
        compiler_params=pltpu.CompilerParams(
            collective_id=0, has_side_effects=True, vmem_limit_bytes=60 * 1024 * 1024
        ),
    )(
        conv_input,
        conv_kernel,
        norm_gain.reshape(1, BLK),
        norm_shift.reshape(1, BLK),
        conv_proj,
        moe_input,
        moe_gain.reshape(1, D),
        routes.T,
        route_weights.T,
        gate_proj,
        up_proj,
        down_proj,
    )


def solution(mesh):
    placed = (
        P("ep", "tp"),
        P(None, "tp"),
        P("tp"),
        P("tp"),
        P("tp", None),
        P(("ep", "tp"), None),
        P(),
        P("ep", None),
        P("ep", None),
        P("ep", None, "tp"),
        P("ep", None, "tp"),
        P("ep", "tp", None),
    )
    return jax.shard_map(
        local,
        mesh=mesh,
        in_specs=placed,
        out_specs=(P(("ep", "tp"), None), P(("ep", "tp"), None)),
        check_vma=False,
    )
```

```python
import jax
import jax.numpy as jnp
from jax import lax
from jax.experimental import pallas as pl
from jax.experimental.pallas import tpu as pltpu
from jax.sharding import PartitionSpec as P

MESH = pl.DeviceIdType.MESH
F32 = jnp.float32
BF16 = jnp.bfloat16

EP = 64
TP = 4
D = 2048
BLK = D // TP
GROUP = 256
TOK = GROUP // TP
CAP = 16
SLOTS = EP * CAP
NCH = 8
CROWS = SLOTS // NCH
CSRC = EP // NCH
HALF = CROWS // 2
ROWS = 1024
QROWS = ROWS // TP
HALO = 32
TAPS = 31
RB = 64
NRB = ROWS // RB
NCB = BLK // 128
PIECE = 64
STEPS_Z = (1, 6, 3, 5, 4, 2, 7, 0)
OWN = 56


def kernel(
    x_hbm, ck_ref, gain_ref, shift_ref, proj_hbm, mi_hbm, mgain_ref, rt_ref, rw_ref, wg_hbm, wu_hbm, wd_hbm,
    cov, mo,
    xb, xf, ckf, mixed, tst, act, actf, proj, mi, wg, wu, wd, nrm, grp, dsp, xg, hid, part, fa, fb,
    rout, rin, rin2, whi, wlo, cmb, fin,
    load_sem, halo_sem, grp_send, grp_recv, st_send, st_recv, dsp_send, dsp_recv,
    act_send, act_recv, w_send, wy, wxl, wxr, wfl, wfr, wc, ag_send, agl, agr, agfl, agfr, rs_send_sem, fal, fbl, ret_send, ret_recv, ret2_send, ret2_recv, fin_send, fin_recv,
):
    g = lax.axis_index("ep")
    y = lax.axis_index("tp")
    right, left, opp = (y + 1) % TP, (y + 3) % TP, (y + 2) % TP
    z, xx, core = g // 8, (g % 8) // 2, g % 2
    ycol = pl.multiple_of(y * BLK, BLK)

    def offsets(i):
        c, j = i // CSRC, i % CSRC
        return STEPS_Z[c], j // 2, j % 2

    zbase = [((z + dz) % 8) * 8 for dz in range(8)]
    xbase = [[((xx + dx) % 4) * 2 + (core + dc) % 2 for dc in range(2)] for dx in range(4)]
    others = [i for i in range(EP) if i != OWN]

    def ahead(i):
        dz, dx, dc = offsets(i)
        return zbase[dz] + xbase[dx][dc]

    def behind(i):
        dz, dx, dc = offsets(i)
        return zbase[-dz % 8] + xbase[-dx % 4][dc]

    def remote(src, dst, send, recv, ep, tp):
        return pltpu.make_async_remote_copy(
            src_ref=src, dst_ref=dst, send_sem=send, recv_sem=recv, device_id=(ep, tp), device_id_type=MESH
        )

    def landed(ref, sem):
        pltpu.make_async_copy(ref, ref, sem).wait()

    loads = [
        pltpu.make_async_copy(mi_hbm, mi, load_sem.at[0]),
        pltpu.make_async_copy(x_hbm, xb.at[pl.ds(HALO, ROWS)], load_sem.at[1]),
        pltpu.make_async_copy(proj_hbm, proj.at[pl.ds(ycol, BLK)], load_sem.at[2]),
        pltpu.make_async_copy(wg_hbm.at[0], wg, load_sem.at[3]),
        pltpu.make_async_copy(wu_hbm.at[0], wu, load_sem.at[4]),
        pltpu.make_async_copy(wd_hbm.at[0], wd, load_sem.at[5]),
    ]
    barrier = pltpu.get_barrier_semaphore()
    for d in range(1, TP):
        pl.semaphore_signal(barrier, inc=1, device_id=(g, (y + d) % TP), device_id_type=MESH)

    loads[0].start()
    for i in others:
        pl.semaphore_signal(barrier, inc=1, device_id=(ahead(i), y), device_id_type=MESH)
    for load in loads[1:]:
        load.start()

    loads[0].wait()
    rows = mi[...].astype(F32)
    scale = lax.rsqrt(jnp.mean(rows * rows, axis=1, keepdims=True) + 1e-6)
    nrm[...] = (rows * scale * mgain_ref[...]).astype(BF16)
    grp[pl.ds(pl.multiple_of(y * TOK, TOK), TOK), :] = nrm[:, pl.ds(ycol, BLK)]

    pl.semaphore_wait(barrier, EP - 1 + TP - 1)

    sends = []
    for d in range(1, TP):
        to = (y + d) % TP
        sends.append(
            remote(
                nrm.at[:, pl.ds(pl.multiple_of(to * BLK, BLK), BLK)],
                grp.at[pl.ds(pl.multiple_of(y * TOK, TOK), TOK), :],
                grp_send.at[d],
                grp_recv.at[d],
                g,
                to,
            )
        )
        sends[-1].start()

    xnext, xprev = zbase[0] + xbase[1][0], zbase[0] + xbase[3][0]
    partner = zbase[0] + xbase[0][1]
    shards = [(y + d) % TP for d in range(1, TP)]

    def shard_rows(t, start, count):
        return proj.at[pl.ds(pl.multiple_of(t * BLK + start, PIECE // 2), count)]

    half_at = core * (BLK // 2)
    piece_at = half_at + xx * PIECE
    def share_y():
        loads[2].wait()
        block = shard_rows(y, piece_at, PIECE)
        remote(block, block, w_send, wy.at[0], g, right).start()
        remote(block, block, w_send, wy.at[1], g, left).start()

    def share_yy():
        landed(proj.at[pl.ds(0, PIECE)], wy.at[0])
        block = shard_rows(left, piece_at, PIECE // 2)
        remote(block, block, w_send, wy.at[2], g, right).start()
        landed(proj.at[pl.ds(0, PIECE)], wy.at[1])
        block = shard_rows(right, piece_at + PIECE // 2, PIECE // 2)
        remote(block, block, w_send, wy.at[3], g, left).start()

    def share_x():
        landed(proj.at[pl.ds(0, PIECE // 2)], wy.at[2])
        landed(proj.at[pl.ds(0, PIECE // 2)], wy.at[3])
        for t in shards:
            block = shard_rows(t, piece_at, PIECE)
            remote(block, block, w_send, wxl, xnext, y).start()
            remote(block, block, w_send, wxr, xprev, y).start()

    def share_xx():
        landed(proj.at[pl.ds(0, 3 * PIECE)], wxl)
        landed(proj.at[pl.ds(0, 3 * PIECE)], wxr)
        for t in shards:
            block = shard_rows(t, half_at + ((xx + 3) % 4) * PIECE, PIECE // 2)
            remote(block, block, w_send, wfl, xnext, y).start()
            block = shard_rows(t, half_at + ((xx + 1) % 4) * PIECE + PIECE // 2, PIECE // 2)
            remote(block, block, w_send, wfr, xprev, y).start()

    def share_core():
        landed(proj.at[pl.ds(0, 3 * PIECE // 2)], wfl)
        landed(proj.at[pl.ds(0, 3 * PIECE // 2)], wfr)
        for t in shards:
            block = shard_rows(t, half_at, BLK // 2)
            remote(block, block, w_send, wc, partner, y).start()

    loads[1].wait()
    halo = remote(xb.at[pl.ds(ROWS, HALO)], xb.at[pl.ds(0, HALO)], halo_sem.at[0], halo_sem.at[1], (g + 1) % EP, y)

    @pl.when(g < EP - 1)
    def _():
        halo.start()

    expert_col = lax.broadcasted_iota(jnp.int32, (EP, GROUP), 0)
    named = (rt_ref[0:1, :] == expert_col) | (rt_ref[1:2, :] == expert_col)
    named_f = jnp.where(named, 1.0, 0.0)
    earlier = lax.broadcasted_iota(jnp.int32, (GROUP, GROUP), 0) < lax.broadcasted_iota(jnp.int32, (GROUP, GROUP), 1)
    rank = jnp.dot(named_f.astype(BF16), jnp.where(earlier, 1.0, 0.0).astype(BF16), preferred_element_type=F32)
    rank = jnp.where(named, rank, -1.0).astype(BF16)
    slot = lax.broadcasted_iota(jnp.int32, (SLOTS, EP), 0)
    spread_rows = jnp.where(slot // CAP == lax.broadcasted_iota(jnp.int32, (SLOTS, EP), 1), 1.0, 0.0).astype(BF16)
    ranks = jnp.dot(spread_rows, rank, preferred_element_type=F32)
    place = (lax.broadcasted_iota(jnp.int32, (SLOTS, GROUP), 0) % CAP).astype(F32)
    chosen = jnp.where(ranks == place, 1.0, 0.0).astype(BF16)
    for d in range(1, TP):
        landed(grp.at[pl.ds(0, TOK), :], grp_recv.at[d])
    dsp[...] = jnp.dot(chosen, grp[...], preferred_element_type=F32).astype(BF16)

    def dispatch(c):
        for i in range(c * CSRC, c * CSRC + CSRC):
            if i != OWN:
                e = ahead(i)
                remote(
                    dsp.at[pl.ds(pl.multiple_of(e * CAP, CAP), CAP), :],
                    xg.at[pl.ds(i * CAP, CAP), pl.ds(ycol, BLK)],
                    dsp_send,
                    dsp_recv.at[c],
                    e,
                    y,
                ).start()

    dispatch(0)
    dispatch(1)
    share_y()
    xg[OWN * CAP : OWN * CAP + CAP, pl.ds(ycol, BLK)] = dsp[pl.ds(pl.multiple_of(g * CAP, CAP), CAP), :]

    def return_rows(c, source, start, target, send, recv):
        for i in range(c * CSRC, c * CSRC + CSRC):
            if i != OWN:
                remote(
                    source.at[pl.ds(start + (i - c * CSRC) * CAP, CAP), :],
                    target.at[pl.ds(pl.multiple_of(g * CAP, CAP), CAP), :],
                    send,
                    recv,
                    behind(i),
                    y,
                ).start()

    def rs_total(c):
        landed(fa.at[c], fal.at[c])
        landed(fb.at[c], fbl.at[c])
        return (part[c, y].astype(F32) + fa[c].astype(F32) + fb[c].astype(F32)).astype(BF16)

    def crows(c):
        return pl.ds(c * CROWS, CROWS)

    def hrows(c, h):
        return pl.ds(c * CROWS + h * HALF, HALF)

    def colof(t):
        return pl.ds(pl.multiple_of(t * BLK, BLK), BLK)

    def gather_start(c):
        landed(xg.at[pl.ds(0, CROWS - CAP if c == OWN // CSRC else CROWS), pl.ds(0, BLK)], dsp_recv.at[c])
        block = xg.at[crows(c), colof(y)]
        remote(block, block, ag_send, agl.at[c], g, right).start()
        remote(block, block, ag_send, agr.at[c], g, left).start()

    def gather_forward(c):
        landed(xg.at[crows(c), colof(left)], agl.at[c])
        piece = xg.at[hrows(c, 0), colof(left)]
        remote(piece, piece, ag_send, agfl.at[c], g, right).start()
        landed(xg.at[crows(c), colof(right)], agr.at[c])
        piece = xg.at[hrows(c, 1), colof(right)]
        remote(piece, piece, ag_send, agfr.at[c], g, left).start()

    def experts(c):
        landed(xg.at[hrows(c, 0), colof(opp)], agfl.at[c])
        landed(xg.at[hrows(c, 1), colof(opp)], agfr.at[c])

        def up(n, carry):
            cols = pl.ds(pl.multiple_of(n * 256, 256), 256)
            rows = xg[crows(c), :]
            gate = jnp.dot(rows, wg[:, cols], preferred_element_type=F32)
            value = jnp.dot(rows, wu[:, cols], preferred_element_type=F32)
            hid[:, cols] = (gate / (1.0 + jnp.exp(-gate)) * value).astype(BF16)
            return carry

        lax.fori_loop(0, BLK // 256, up, 0)

        def down(q):
            part[c, q] = jnp.dot(hid[...], wd[:, colof(q)], preferred_element_type=F32).astype(BF16)

        down(right)
        remote(part.at[c, right], fa.at[c], rs_send_sem, fal.at[c], g, right).start()
        down(left)
        remote(part.at[c, left], fb.at[c], rs_send_sem, fbl.at[c], g, left).start()
        down(opp)
        return_rows(c, part.at[c, opp], 0, rin2, ret2_send, ret2_recv)
        if c == OWN // CSRC:
            rin2[pl.ds(pl.multiple_of(g * CAP, CAP), CAP), :] = part[c, opp, 0:CAP, :]
        down(y)

    def give_back(c):
        rout[crows(c), :] = rs_total(c)

        return_rows(c, rout, c * CROWS, rin, ret_send, ret_recv)
        if c == OWN // CSRC:
            rin[pl.ds(pl.multiple_of(g * CAP, CAP), CAP), :] = rout[OWN * CAP : OWN * CAP + CAP, :]

    def conv_out(first, last):
        def columns(n, carry):
            cols = pl.ds(pl.multiple_of(n * 256, 256), 256)
            cov[:, cols] = jnp.dot(actf[...], proj[:, cols], preferred_element_type=F32).astype(BF16)
            return carry

        lax.fori_loop(first, last, columns, 0)

    for cb in range(NCB):
        ckf[cb, 0:TAPS, :] = ck_ref[:, cb * 128 : cb * 128 + 128].astype(F32)

    def widen(b, carry):
        r = pl.multiple_of(HALO + b * 64, 32)
        for cb in range(NCB):
            xf[cb, pl.ds(r, 64), :] = xb[pl.ds(r, 64), cb * 128 : cb * 128 + 128].astype(F32)
        return carry

    lax.fori_loop(0, ROWS // 64, widen, 0)

    lane = lax.broadcasted_iota(jnp.int32, (RB, 128), 1)

    def conv_rows(rb, carry):
        base = pl.multiple_of(rb * RB, RB)
        total = jnp.zeros((RB, 128), F32)
        squares = jnp.zeros((RB, 128), F32)
        for cb in range(NCB):
            acc = jnp.zeros((RB, 128), F32)
            for tap in range(TAPS):
                acc = acc + xf[cb, pl.ds(base + (2 + tap), RB), :] * ckf[cb, tap : tap + 1, :]
            mixed[cb, pl.ds(base, RB), :] = acc
            total = total + acc
            squares = squares + acc * acc
        stats = jnp.where(lane == rb, jnp.sum(total, axis=1, keepdims=True), tst[TP])
        tst[TP] = jnp.where(lane == rb + NRB, jnp.sum(squares, axis=1, keepdims=True), stats)
        return carry

    def conv_span(first, last):
        lax.fori_loop(first, last, conv_rows, 0)

    def conv_last():
        @pl.when(g > 0)
        def _():
            halo.wait_recv()

        @pl.when(g == 0)
        def _():
            xb[0:HALO, :] = jnp.zeros((HALO, BLK), BF16)

        for cb in range(NCB):
            xf[cb, 0:HALO, :] = xb[0:HALO, cb * 128 : cb * 128 + 128].astype(F32)
        conv_span(0, 1)
        for d in range(1, TP):
            to = (y + d) % TP
            stat_sends.append(remote(tst.at[TP], tst.at[y], st_send.at[d], st_recv.at[d], g, to))
            stat_sends[-1].start()

    def activate_span(first, last):
        means = (tst[TP] + tst[right] + tst[opp] + tst[left]) * (1.0 / D)

        def activate(rb, carry):
            base = pl.multiple_of(rb * RB, RB)
            center = jnp.sum(jnp.where(lane == rb, means, 0.0), axis=1, keepdims=True)
            square = jnp.sum(jnp.where(lane == rb + NRB, means, 0.0), axis=1, keepdims=True)
            inv = lax.rsqrt(jnp.maximum(square - center * center, 0.0) + 1e-5)
            for cb in range(NCB):
                cols = slice(cb * 128, cb * 128 + 128)
                v = (mixed[cb, pl.ds(base, RB), :] - center) * inv * gain_ref[:, cols] + shift_ref[:, cols]
                act[pl.ds(base, RB), cols] = (v / (1.0 + jnp.exp(-v))).astype(BF16)
            return carry

        lax.fori_loop(first, last, activate, 0)

    def share_act(d):
        to = (y + d) % TP
        remote(
            act.at[pl.ds(pl.multiple_of(to * QROWS, QROWS), QROWS)],
            actf.at[:, pl.ds(ycol, BLK)],
            act_send,
            act_recv.at[d],
            g,
            to,
        ).start()

    stat_sends = []
    tst[TP] = jnp.zeros((RB, 128), F32)
    pick = lax.broadcasted_iota(jnp.int32, (128, GROUP), 0)
    table = jnp.where(pick == 0, rt_ref[0:1, :].astype(F32), 0.0)
    table = jnp.where(pick == 1, rt_ref[1:2, :].astype(F32), table)
    table = jnp.where(pick == 2, rw_ref[0:1, :], table)
    table = jnp.where(pick == 3, rw_ref[1:2, :], table)
    table = jnp.transpose(table)
    expert_lane = lax.broadcasted_iota(jnp.int32, (GROUP, EP), 1).astype(F32)
    first = table[:, 0:1] == expert_lane
    second = table[:, 1:2] == expert_lane
    named_t = jnp.where(first | second, 1.0, 0.0)
    before = lax.broadcasted_iota(jnp.int32, (GROUP, GROUP), 1) < lax.broadcasted_iota(jnp.int32, (GROUP, GROUP), 0)
    rank_t = jnp.dot(jnp.where(before, 1.0, 0.0).astype(BF16), named_t.astype(BF16), preferred_element_type=F32)
    rank_t = jnp.where(first | second, rank_t, -1.0).astype(BF16)
    weight_t = jnp.where(first, table[:, 2:3], 0.0) + jnp.where(second, table[:, 3:4], 0.0)
    weight_hi = weight_t.astype(BF16)
    weight_lo = (weight_t - weight_hi.astype(F32)).astype(BF16)
    slot_lane = lax.broadcasted_iota(jnp.int32, (EP, SLOTS), 1)
    spread_cols = jnp.where(slot_lane // CAP == lax.broadcasted_iota(jnp.int32, (EP, SLOTS), 0), 1.0, 0.0).astype(BF16)
    hit = jnp.dot(rank_t, spread_cols, preferred_element_type=F32) == (
        lax.broadcasted_iota(jnp.int32, (GROUP, SLOTS), 1) % CAP
    ).astype(F32)
    whi[...] = jnp.where(hit, jnp.dot(weight_hi, spread_cols, preferred_element_type=F32), 0.0).astype(BF16)
    wlo[...] = jnp.where(hit, jnp.dot(weight_lo, spread_cols, preferred_element_type=F32), 0.0).astype(BF16)

    conv_span(1, 4)
    gather_start(0)
    dispatch(2)
    dispatch(3)
    dispatch(4)
    share_yy()
    gather_forward(0)
    gather_start(1)
    dispatch(5)
    dispatch(6)
    dispatch(7)
    for load in loads[3:]:
        load.wait()
    conv_span(4, 6)
    for k in range(NCH):
        experts(k)
        if k + 1 < NCH:
            gather_forward(k + 1)
        if k + 2 < NCH:
            gather_start(k + 2)
        if k == 0:
            share_x()
        if k >= 1:
            give_back(k - 1)
        if k < 3:
            conv_span(6 + 3 * k, 9 + 3 * k)
        if k == 3:
            conv_span(15, 16)
            conv_last()
        if k == NCH - 3:
            share_xx()
            for d in range(1, TP):
                landed(tst.at[0], st_recv.at[d])
            activate_span(0, NRB // 2)
        if k == NCH - 2:
            activate_span(NRB // 2, NRB)
        if k == NCH - 1:
            share_core()
    give_back(NCH - 1)
    share_act(2)
    share_act(1)
    share_act(3)
    actf[:, pl.ds(ycol, BLK)] = act[pl.ds(pl.multiple_of(y * QROWS, QROWS), QROWS), :]

    def combine(rows):
        total = jnp.dot(whi[...], rows[...], preferred_element_type=F32)
        return (total + jnp.dot(wlo[...], rows[...], preferred_element_type=F32)).astype(BF16)

    def to_owners(half):
        for d in (2, 1, 3):
            to = (y + d) % TP
            sends.append(
                remote(
                    cmb.at[half, pl.ds(pl.multiple_of(to * TOK, TOK), TOK), :],
                    fin.at[half, y],
                    fin_send.at[d + 4 * half],
                    fin_recv.at[d + 4 * half],
                    g,
                    to,
                )
            )
            sends[-1].start()
        fin[half, y] = cmb[half, pl.ds(pl.multiple_of(y * TOK, TOK), TOK), :]

    landed(rin2.at[pl.ds(0, SLOTS - CAP), :], ret2_recv)
    cmb[1] = combine(rin2)
    to_owners(1)
    landed(rin.at[pl.ds(0, SLOTS - CAP), :], ret_recv)
    cmb[0] = combine(rin)
    to_owners(0)
    landed(proj.at[pl.ds(0, 3 * (BLK // 2))], wc)
    for d in range(1, TP):
        landed(actf.at[:, pl.ds(0, BLK)], act_recv.at[d])
    conv_out(0, 8)

    for d in range(1, TP):
        landed(fin.at[0, 0], fin_recv.at[d])
        landed(fin.at[0, 0], fin_recv.at[d + 4])
    for t in range(TP):
        both = fin[0, t].astype(F32) + fin[1, (t + 2) % TP].astype(F32)
        mo[:, t * BLK : t * BLK + BLK] = both.astype(BF16)

    for send in sends + stat_sends:
        send.wait_send()

    @pl.when(g < EP - 1)
    def _():
        halo.wait_send()

    landed(dsp.at[pl.ds(0, SLOTS - CAP), :], dsp_send)
    landed(rout.at[pl.ds(0, SLOTS - CAP), :], ret_send)
    landed(xg.at[pl.ds(0, 3 * SLOTS // TP), :], ag_send)
    landed(part.at[:, pl.ds(0, 2)], rs_send_sem)
    landed(rout.at[pl.ds(0, SLOTS - CAP), :], ret2_send)
    landed(act.at[pl.ds(0, 3 * QROWS)], act_send)
    landed(proj.at[pl.ds(0, 24 * PIECE)], w_send)


def local(
    conv_input, conv_kernel, norm_gain, norm_shift, conv_proj, moe_input, moe_gain, routes, route_weights,
    gate_proj, up_proj, down_proj,
):
    vmem = pl.BlockSpec(memory_space=pltpu.VMEM)
    hbm = pl.BlockSpec(memory_space=pl.ANY)
    dma, jobs = pltpu.SemaphoreType.DMA, NCH
    v = pltpu.VMEM
    return pl.pallas_call(
        kernel,
        out_shape=(
            pltpu.VMEM((QROWS, D), BF16),
            pltpu.VMEM((TOK, D), BF16),
        ),
        in_specs=[hbm, vmem, vmem, vmem, hbm, hbm, vmem, vmem, vmem, hbm, hbm, hbm],
        out_specs=(vmem, vmem),
        scratch_shapes=[
            v((HALO + ROWS, BLK), BF16),
            v((NCB, HALO + ROWS, 128), F32),
            v((NCB, 32, 128), F32),
            v((NCB, ROWS, 128), F32),
            v((TP + 1, RB, 128), F32),
            v((ROWS, BLK), BF16),
            v((QROWS, D), BF16),
            v((D, D), BF16),
            v((TOK, D), BF16),
            v((D, BLK), BF16),
            v((D, BLK), BF16),
            v((BLK, D), BF16),
            v((TOK, D), BF16),
            v((GROUP, BLK), BF16),
            v((SLOTS, BLK), BF16),
            v((SLOTS, D), BF16),
            v((CROWS, BLK), BF16),
            v((jobs, TP, CROWS, BLK), BF16),
            v((jobs, CROWS, BLK), BF16),
            v((jobs, CROWS, BLK), BF16),
            v((SLOTS, BLK), BF16),
            v((SLOTS, BLK), BF16),
            v((SLOTS, BLK), BF16),
            v((GROUP, SLOTS), BF16),
            v((GROUP, SLOTS), BF16),
            v((2, GROUP, BLK), BF16),
            v((2, TP, TOK, BLK), BF16),
            dma((6,)),
            dma((2,)),
            dma((TP,)),
            dma((TP,)),
            dma((TP,)),
            dma((TP,)),
            dma,
            dma((NCH,)),
            dma,
            dma((TP,)),
            dma,
            dma((TP,)),
            dma,
            dma,
            dma,
            dma,
            dma,
            dma,
            dma((NCH,)),
            dma((NCH,)),
            dma((NCH,)),
            dma((NCH,)),
            dma,
            dma((jobs,)),
            dma((jobs,)),
            dma,
            dma,
            dma,
            dma,
            dma((8,)),
            dma((8,)),
        ],
        compiler_params=pltpu.CompilerParams(
            collective_id=0, has_side_effects=True, vmem_limit_bytes=60 * 1024 * 1024
        ),
    )(
        conv_input,
        conv_kernel,
        norm_gain.reshape(1, BLK),
        norm_shift.reshape(1, BLK),
        conv_proj,
        moe_input,
        moe_gain.reshape(1, D),
        routes.T,
        route_weights.T,
        gate_proj,
        up_proj,
        down_proj,
    )


def solution(mesh):
    placed = (
        P("ep", "tp"),
        P(None, "tp"),
        P("tp"),
        P("tp"),
        P("tp", None),
        P(("ep", "tp"), None),
        P(),
        P("ep", None),
        P("ep", None),
        P("ep", None, "tp"),
        P("ep", None, "tp"),
        P("ep", "tp", None),
    )
    return jax.shard_map(
        local,
        mesh=mesh,
        in_specs=placed,
        out_specs=(P(("ep", "tp"), None), P(("ep", "tp"), None)),
        check_vma=False,
    )
```
